512 devices in a mesh: sp: 16 (over z), fs: 4 (over y), tp: 8 (over x, core).
Axes of the slice: x: 4, y: 4, z: 16, core: 2. Of those that a mesh axis runs over, the one named last changes fastest.
Arguments:
- tokens: bfloat16 [16384, 2048], P(('fs', 'sp', 'tp')), parts along dimension 0, may hold values from -6 to 6
- norm_gain: bfloat16 [2048], replicated, may hold values from 0.099609375 to 1.8984375
- w_pool_in: bfloat16 [2048, 1024], P('sp', 'tp'), may hold values from -0.125 to 0.125
- w_query: bfloat16 [2048, 1024], P('sp', 'tp'), may hold values from -0.125 to 0.125
- w_key: bfloat16 [2048, 1024], P('sp', 'tp'), may hold values from -0.125 to 0.125
- w_value: bfloat16 [2048, 1024], P('sp', 'tp'), may hold values from -0.125 to 0.125
- w_gate: bfloat16 [2048, 1024], P('sp', 'tp'), may hold values from -0.125 to 0.125
- w_beta: bfloat16 [2048, 8], replicated, may hold values from -0.125 to 0.125
- w_decay: bfloat16 [2048, 8], replicated, may hold values from -0.5 to 0.5
- conv_weight: float32 [3, 4, 1024], P(None, None, 'tp'), may hold values from -3 to 3
- a_log: float32 [8], P('tp'), may hold values from -20 to -1.7, as said below
- decay_extra: float32 [16384, 8], P(('fs', 'sp'), 'tp'), parts along dimension 0, may hold values from -1.4 to 0
- w_mix: bfloat16 [8, 128, 128], P('tp'), may hold values from -0.5 to 0.5
- pool_scale: float32 [1024], P('tp'), may hold values from 0.1 to 1.9
- delta_gain: float32 [128], replicated, may hold values from 0.1 to 1.9
- w_out_pool: bfloat16 [1024, 2048], P('tp', 'sp'), may hold values from -0.125 to 0.125
- w_out_delta: bfloat16 [1024, 2048], P('tp', 'sp'), may hold values from -0.125 to 0.125
Outputs:
- mixed: bfloat16 [16384, 2048], P(('fs', 'sp', 'tp')), parts along dimension 0
The draws below stay inside these ranges and needn't reach their ends.
There are 4 independent parts, one for each index of `fs`. The reference program is written for one: setup_inputs(seed, part) draws one part's arguments, and reference() takes and returns one part's arrays. A program takes and returns all parts, laid end to end along the dimension named above; an argument that names none is the same for every part. Nothing has to cross between parts.
Inputs may be any that keep to these rules, and one draw needn't show every extreme that they name: `a_log`: logarithm of each head's base decay rate.
All inputs are finite; a program needn't handle non-finite values.
Results may differ from the reference program's by a relative error of at most 0.018.
Values may be sent and summed in bfloat16 or wider, within the bound.
No kernel may reach another device: no remote copies, remote signals or barrier semaphores. Data moves between devices by JAX's collectives and lax.ppermute only.
A program may use at most 64 MiB of HBM per device.

```python
import jax
import jax.numpy as jnp
from jax import lax

D = 2048
POOL_GROUPS = 8
GROUP_DIM = 128
DN_HEADS = 8
HEAD_DIM = 128
CONV = 4
BLOCK = 64
SP_TOK = 256
POOL_WIDTH = 1024
DN_WIDTH = 1024
SEQ = 4096
N_TP = 8


def draw_a_log(key, part):
    chooser, slow_key, fast_key = jax.random.split(jax.random.fold_in(key, 11), 3)
    fast_share = 0.5
    fast = jax.random.uniform(chooser, (DN_HEADS,), jnp.float32) < fast_share
    slow_rate = jnp.exp(jax.random.uniform(slow_key, (DN_HEADS,), jnp.float32, jnp.log(0.05), jnp.log(0.2))) / SEQ
    fast_rate = jax.random.uniform(fast_key, (DN_HEADS,), jnp.float32, 1.0 / 16.0, 1.0 / 6.0)
    return jnp.log(jnp.where(fast, fast_rate, slow_rate)).astype(jnp.float32)


def draw_decay_extra(key, part):
    rate_key, position_seed, depth_key = jax.random.split(jax.random.fold_in(key, 23), 3)
    rates = jnp.exp(jax.random.uniform(rate_key, (SEQ // SP_TOK, DN_HEADS), jnp.float32, jnp.log(0.1), jnp.log(0.6))) / SEQ
    starting_shift = -jnp.repeat(rates, SP_TOK, axis=0)
    places = jax.random.randint(position_seed, (2, DN_HEADS), 0, SEQ)
    layer_ordinal = jax.random.uniform(depth_key, (2, DN_HEADS), jnp.float32, 0.22, 0.69)
    positions = jnp.arange(SEQ, dtype=jnp.int32)
    agreeing_tally = (positions[:, None, None] == places[None, :, :]).astype(jnp.float32)
    window_bundles = -jnp.sum(agreeing_tally * layer_ordinal[None, :, :], axis=1)
    return (starting_shift + window_bundles).astype(jnp.float32)


def shard_levels(own_key, shape, shards, smallest, high):
    loudness = 1.0
    for position, parts in shards:
        heights = jax.random.uniform(jax.random.fold_in(jax.random.fold_in(own_key, 6), position), (parts,), jnp.float32, smallest / len(shards), high / len(shards))
        loudness = loudness * jnp.repeat(jnp.exp(heights), shape[position] // parts).reshape((-1,) + (1,) * (len(shape) - 1 - position))
    return loudness


def centred(stream_key, shape, scale, most, shards=(), kind=jnp.bfloat16):
    values = scale * jax.random.normal(stream_key, shape, jnp.float32)
    if shards:
        values = values * shard_levels(stream_key, shape, shards, -0.22, 0.18)
    return jnp.clip(values, -most, most).astype(kind)


def setup_inputs(seed: int = 0, part: int = 0) -> dict:
    seeds = jax.random.split(jax.random.key(seed), 18)
    part_keys = jax.random.split(jax.random.fold_in(seeds[17], part), 18)
    return {
        "tokens": centred(part_keys[0], (SEQ, D), 1.0, 6.0, ((0, 128),)),
        "norm_gain": jnp.clip(1.0 + 0.18 * jax.random.normal(seeds[1], (D,), jnp.float32), 0.099609375, 1.8984375).astype(jnp.bfloat16),
        "w_pool_in": centred(seeds[2], (D, POOL_WIDTH), D ** -0.5, 0.125, ((0, 16), (1, 8))),
        "w_query": centred(seeds[3], (D, DN_WIDTH), D ** -0.5, 0.125, ((0, 16), (1, 8))),
        "w_key": centred(seeds[4], (D, DN_WIDTH), D ** -0.5, 0.125, ((0, 16), (1, 8))),
        "w_value": centred(seeds[5], (D, DN_WIDTH), D ** -0.5, 0.125, ((0, 16), (1, 8))),
        "w_gate": centred(seeds[6], (D, DN_WIDTH), D ** -0.5, 0.125, ((0, 16), (1, 8))),
        "w_beta": centred(seeds[7], (D, DN_HEADS), D ** -0.5, 0.125),
        "w_decay": centred(seeds[8], (D, DN_HEADS), (D // 16) ** -0.5, 0.5),
        "conv_weight": centred(seeds[9], (3, CONV, DN_WIDTH), CONV ** -0.5, 3.0, ((2, 8),), jnp.float32),
        "a_log": draw_a_log(jax.random.fold_in(seeds[17], 71), part),
        "decay_extra": draw_decay_extra(jax.random.fold_in(jax.random.fold_in(seeds[17], part), 71), part),
        "w_mix": centred(seeds[12], (POOL_GROUPS, GROUP_DIM, GROUP_DIM), GROUP_DIM ** -0.5, 0.5, ((0, 8),)),
        "pool_scale": jnp.clip(1.0 + 0.18 * jax.random.normal(seeds[13], (POOL_WIDTH,), jnp.float32), 0.1, 1.9),
        "delta_gain": jnp.clip(1.0 + 0.18 * jax.random.normal(seeds[14], (HEAD_DIM,), jnp.float32), 0.1, 1.9),
        "w_out_pool": centred(seeds[15], (POOL_WIDTH, D), (POOL_WIDTH + DN_WIDTH) ** -0.5, 0.125, ((0, 8), (1, 16))),
        "w_out_delta": centred(seeds[16], (DN_WIDTH, D), (POOL_WIDTH + DN_WIDTH) ** -0.5, 0.125, ((0, 8), (1, 16))),
    }


eps = 1e-06
windows = (2, 4, 8, 16)
highest = lax.Precision.HIGHEST

def rms_rows(values, gain):
    floats = values.astype(jnp.float32)
    scale = lax.rsqrt(lax.optimization_barrier(jnp.mean(floats * floats, axis=-1, keepdims=True)) + eps)
    return (floats * scale * gain.astype(jnp.float32)).astype(jnp.bfloat16)

def unit_rows(values):
    return values * lax.rsqrt(lax.optimization_barrier(jnp.sum(values * values, axis=-1, keepdims=True)) + eps)

def block_terms(query, keys, values, log_gate, strength, block):
    heads, length, width = keys.shape
    count = length // block

    def split(tensor):
        return tensor.reshape(heads, count, block, tensor.shape[-1])
    query_part, key_part, value_part = (split(query), split(keys), split(values))
    gate_cum = jnp.cumsum(log_gate.reshape(heads, count, block), axis=-1)
    beta_part = strength.reshape(heads, count, block)[..., None]
    lower_mask = jnp.tril(jnp.ones((block, block), dtype=bool))
    strict_mask = jnp.tril(jnp.ones((block, block), dtype=bool), k=-1)
    gaps = gate_cum[..., :, None] - gate_cum[..., None, :]
    decay_tab = jnp.where(lower_mask, jnp.exp(jnp.where(lower_mask, gaps, 0.0)), 0.0)
    key_scaled_beta = key_part * beta_part
    value_beta = value_part * beta_part
    corr_lower = jnp.where(strict_mask, jnp.einsum('hnid,hnjd->hnij', key_scaled_beta, key_part, precision=highest) * decay_tab, 0.0)
    identity = jnp.eye(block, dtype=jnp.float32)
    inverse = lax.linalg.triangular_solve(identity + corr_lower, jnp.broadcast_to(identity, corr_lower.shape), left_side=True, lower=True)
    fixed_values = jnp.einsum('hnij,hnjd->hnid', inverse, value_beta, precision=highest)
    key_weights = jnp.einsum('hnij,hnjd->hnid', inverse, key_scaled_beta * jnp.exp(gate_cum)[..., None], precision=highest)
    scores = jnp.where(lower_mask, jnp.einsum('hnid,hnjd->hnij', query_part, key_part, precision=highest) * decay_tab, 0.0)
    key_decayed = key_part * jnp.exp(gate_cum[..., -1:] - gate_cum)[..., None]
    query_gated = query_part * jnp.exp(gate_cum)[..., None]
    terms = (query_gated, key_decayed, fixed_values, key_weights, scores, gate_cum[..., -1])
    return tuple((jnp.moveaxis(tensor, 1, 0) for tensor in terms))

def carry_step(state, inputs):
    query_gated, key_decayed, fixed_values, key_weights, scores, last_gate = inputs
    fresh = fixed_values - jnp.einsum('hcd,hde->hce', key_weights, state, precision=highest)
    output = jnp.einsum('hcd,hde->hce', query_gated, state, precision=highest) + jnp.einsum('hij,hje->hie', scores, fresh, precision=highest)
    state = state * jnp.exp(last_gate)[:, None, None] + jnp.einsum('hcd,hce->hde', key_decayed, fresh, precision=highest)
    return (state, output)

def reference(tokens, norm_gain, w_pool_in, w_query, w_key, w_value, w_gate, w_beta, w_decay, conv_weight, a_log, decay_extra, w_mix, pool_scale, delta_gain, w_out_pool, w_out_delta):
    norm_result = rms_rows(tokens, norm_gain)

    def project(weight):
        return jnp.dot(norm_result.astype(jnp.float32), weight.astype(jnp.float32), preferred_element_type=jnp.float32).astype(jnp.bfloat16)
    pool_in = project(w_pool_in)
    query_raw = project(w_query)
    key_raw = project(w_key)
    value_raw = project(w_value)
    gate_raw = project(w_gate)
    beta_pre = jnp.dot(norm_result.astype(jnp.float32), w_beta.astype(jnp.float32), preferred_element_type=jnp.float32)
    forget_logits = jnp.dot(norm_result.astype(jnp.float32), w_decay.astype(jnp.float32), preferred_element_type=jnp.float32)
    source_rows = pool_in.astype(jnp.float32)
    running = jnp.concatenate([jnp.zeros((1, POOL_WIDTH), jnp.float32), jnp.cumsum(source_rows, axis=0)], axis=0)
    group = (jnp.arange(POOL_WIDTH) // GROUP_DIM).astype(jnp.int32)
    span = (2 ** (1 + group % 4)).astype(jnp.int32)
    window_sum = jnp.zeros((SEQ, POOL_WIDTH), jnp.float32)
    for width in windows:
        lagged = jnp.concatenate([jnp.zeros((width - 1, POOL_WIDTH), jnp.float32), running[:SEQ - width + 1]], axis=0)
        window_sum = window_sum + jnp.where(span[None, :] == width, running[1:] - lagged, 0.0)
    positions = jnp.arange(SEQ).astype(jnp.int32)
    counts = jnp.minimum(positions[:, None] + 1, span[None, :]).astype(jnp.float32)
    pooled = (window_sum / counts - source_rows).astype(jnp.bfloat16)
    mixed_pool = jnp.einsum('sgc,gcd->sgd', pooled.reshape(SEQ, POOL_GROUPS, GROUP_DIM).astype(jnp.float32), w_mix.astype(jnp.float32), precision=highest)
    pool_out = (mixed_pool.reshape(SEQ, POOL_WIDTH) * pool_scale).astype(jnp.bfloat16)
    stacked = jnp.concatenate([query_raw, key_raw, value_raw], axis=1).astype(jnp.float32)
    kernel = jnp.transpose(conv_weight, (1, 0, 2)).reshape(CONV, 3 * DN_WIDTH)
    padded = jnp.concatenate([jnp.zeros((CONV - 1, 3 * DN_WIDTH), jnp.float32), stacked], axis=0)
    conv = jnp.zeros((SEQ, 3 * DN_WIDTH), jnp.float32)
    for tap in range(CONV):
        conv = conv + padded[tap:tap + SEQ] * kernel[tap]
    after_silu = jax.nn.silu(conv)

    def heads_first(tensor):
        return jnp.transpose(tensor.reshape(SEQ, DN_HEADS, HEAD_DIM), (1, 0, 2))
    query = unit_rows(heads_first(after_silu[:, :DN_WIDTH])) * HEAD_DIM ** (-0.5)
    keys = unit_rows(heads_first(after_silu[:, DN_WIDTH:2 * DN_WIDTH]))
    values = heads_first(after_silu[:, 2 * DN_WIDTH:])
    strength = jax.nn.sigmoid(beta_pre).T
    log_gate = (-jnp.exp(a_log)[None, :] * jax.nn.softplus(forget_logits) + decay_extra).T
    terms = block_terms(query, keys, values, log_gate, strength, BLOCK)
    _, outputs = lax.scan(carry_step, jnp.zeros((DN_HEADS, HEAD_DIM, HEAD_DIM), jnp.float32), terms)
    attended = jnp.transpose(outputs, (1, 0, 2, 3)).reshape(DN_HEADS, SEQ, HEAD_DIM)
    normal_out = attended * lax.rsqrt(lax.optimization_barrier(jnp.mean(attended * attended, axis=-1, keepdims=True)) + eps) * delta_gain
    gated = normal_out * jax.nn.silu(heads_first(gate_raw.astype(jnp.float32)))
    delta_out = jnp.transpose(gated, (1, 0, 2)).reshape(SEQ, DN_WIDTH).astype(jnp.bfloat16)
    pool_cols = POOL_WIDTH // N_TP
    delta_cols = DN_WIDTH // N_TP
    total = jnp.zeros((SEQ, D), jnp.float32)
    for lane in range(N_TP):
        value_partial_rows = jnp.dot(pool_out[:, lane * pool_cols:(lane + 1) * pool_cols].astype(jnp.float32), w_out_pool[lane * pool_cols:(lane + 1) * pool_cols].astype(jnp.float32), preferred_element_type=jnp.float32)
        value_partial_rows = value_partial_rows + jnp.dot(delta_out[:, lane * delta_cols:(lane + 1) * delta_cols].astype(jnp.float32), w_out_delta[lane * delta_cols:(lane + 1) * delta_cols].astype(jnp.float32), preferred_element_type=jnp.float32)
        total = total + lax.optimization_barrier(value_partial_rows.astype(jnp.bfloat16)).astype(jnp.float32)
    return total.astype(jnp.bfloat16)
```

```python
import functools

import jax
import jax.numpy as jnp
from jax import lax
from jax.experimental import pallas as pl
from jax.experimental.pallas import tpu as pltpu
from jax.sharding import PartitionSpec as P

EPS = 1e-06
HALO = 16
F32 = jnp.float32
BF16 = jnp.bfloat16


def call(kernel, outs, *args, smem=0, scratch=(), flops=0):
    in_specs = [pl.BlockSpec(memory_space=pltpu.SMEM)] * smem + [
        pl.BlockSpec(memory_space=pltpu.VMEM)
    ] * (len(args) - smem)
    many = isinstance(outs, (list, tuple))
    out_specs = pl.BlockSpec(memory_space=pltpu.VMEM)
    return pl.pallas_call(
        kernel,
        out_shape=list(outs) if many else outs,
        in_specs=in_specs,
        out_specs=[out_specs] * len(outs) if many else out_specs,
        scratch_shapes=list(scratch),
        cost_estimate=pl.CostEstimate(flops=flops, bytes_accessed=0, transcendentals=0),
        name=kernel.__name__ if hasattr(kernel, "__name__") else kernel.func.__name__,
    )(*args)


def shape(*dims, dtype=F32):
    return jax.ShapeDtypeStruct(dims, dtype)


def dot(a, b, dims=((1,), (0,))):
    return lax.dot_general(a, b, (dims, ((), ())), preferred_element_type=F32)


def split(a):
    high = a.astype(BF16)
    return high, (a - high.astype(F32)).astype(BF16)


def dot3(a, b, dims=((1,), (0,))):
    ah, al = split(a)
    bh, bl = split(b)
    return dot(ah, bh, dims) + (dot(ah, bl, dims) + dot(al, bh, dims))


def pack_first(f_ref, a_ref, b_ref, out_ref):
    half = a_ref.shape[0] // 2
    rows = pl.ds(pl.multiple_of((f_ref[0] % 2) * half, half), half)
    piece = jnp.where(f_ref[0] < 2, a_ref[rows, :], b_ref[rows, :])
    for i in range(out_ref.shape[0]):
        out_ref[i] = piece


def pack_rest(f_ref, q_ref, g_ref, p_ref, op_ref, od_ref, qg_ref, poo_ref, stacked):
    pack_first(f_ref, q_ref, g_ref, qg_ref)
    n = p_ref.shape[0]
    stacked[0:n] = p_ref[...]
    stacked[n : 2 * n] = op_ref[...]
    stacked[2 * n : 3 * n] = od_ref[...]
    part = 3 * n // 4
    piece = stacked[pl.ds(pl.multiple_of(f_ref[0] * part, 32), part), :]
    for i in range(poo_ref.shape[0]):
        poo_ref[i] = piece


def everyone(x, axis):
    return jnp.broadcast_to(x, (lax.axis_size(axis), *x.shape))


def exchange(copies, axis, groups=None):
    return lax.all_to_all(
        copies, axis, split_axis=0, concat_axis=0, tiled=True, axis_index_groups=groups
    )


def norm_kernel(
    ids_ref, a_log_ref, tok_ref, tail_ref, gain_ref, wbd_ref, extra_ref,
    xn_ref, beta_ref, gc_ref, decay_ref,
):
    length = tok_ref.shape[0]
    gain = gain_ref[...].astype(F32)

    def rms(rows):
        x = rows.astype(F32)
        scale = lax.rsqrt(jnp.mean(x * x, axis=-1, keepdims=True) + EPS)
        return (x * scale * gain).astype(BF16)

    tail = rms(tail_ref[...])
    xn_ref[0:HALO] = jnp.where(ids_ref[0] > 0, tail, jnp.zeros_like(tail))
    step = 64
    for i in range(length // step):
        xn_ref[HALO + i * step : HALO + (i + 1) * step] = rms(tok_ref[i * step : (i + 1) * step])
    pre = dot(xn_ref[HALO:], wbd_ref[...], ((1,), (1,)))
    heads = pre.shape[1] // 2
    col = lax.broadcasted_iota(jnp.int32, pre.shape, 1)
    lane = ids_ref[1]
    beta_pre = jnp.sum(jnp.where(col == lane, pre, 0.0), axis=1, keepdims=True)
    decay_pre = jnp.sum(jnp.where(col == lane + heads, pre, 0.0), axis=1, keepdims=True)
    wide = (length, 128)
    beta_ref[...] = jax.nn.sigmoid(jnp.broadcast_to(beta_pre, wide))
    rate = jnp.exp(jnp.full(wide, a_log_ref[0], F32))
    soft = jax.nn.softplus(jnp.broadcast_to(decay_pre, wide))
    log_gate = -rate * soft + jnp.broadcast_to(extra_ref[...], wide)
    r = lax.broadcasted_iota(jnp.int32, (length, length), 0)
    c = lax.broadcasted_iota(jnp.int32, (length, length), 1)
    lower = jnp.where(r >= c, 1.0, 0.0).astype(BF16)
    g1 = log_gate.astype(BF16)
    rest = log_gate - g1.astype(F32)
    g2 = rest.astype(BF16)
    g3 = (rest - g2.astype(F32)).astype(BF16)
    gc = dot(lower, g1) + (dot(lower, g2) + dot(lower, g3))
    gc_ref[...] = gc
    across = jnp.transpose(gc)
    across = jnp.concatenate([across] * (length // 128), axis=0)
    along = jnp.concatenate([gc] * (length // 128), axis=1)
    gaps = along - across
    decay_ref[...] = jnp.where(r >= c, jnp.exp(jnp.where(r >= c, gaps, 0.0)), 0.0)


def gather_two(w_ref, w_scr):
    _, count, half, width = w_ref.shape
    for m in range(2):
        for s in range(count):
            for h in range(2):
                at = (2 * s + h) * half
                w_scr[at : at + half, m * width : (m + 1) * width] = w_ref[2 * m + h, s]


def short_conv(raw, taps, length, x_scr):
    x_scr[...] = raw.astype(BF16).astype(F32)
    conv = jnp.zeros((length, raw.shape[1]), F32)
    for j in range(4):
        conv = conv + x_scr[HALO - 3 + j : HALO - 3 + j + length, :] * taps[j : j + 1, :]
    return jax.nn.silu(conv)


def unit_rows(x):
    return x * lax.rsqrt(jnp.sum(x * x, axis=-1, keepdims=True) + EPS)


def inverse_unit_lower(low, size):
    r = lax.broadcasted_iota(jnp.int32, (size, size), 0)
    c = lax.broadcasted_iota(jnp.int32, (size, size), 1)
    inv = [jnp.where(r == c, 1.0, 0.0) - jnp.where((r // 2 == c // 2) & (r > c), x, 0.0) for x in low]
    b = 2
    while b < size:
        mask = (r // (2 * b) == c // (2 * b)) & (r % (2 * b) >= b) & (c % (2 * b) < b)
        mid = [dot3(x, jnp.where(mask, y, 0.0)) for x, y in zip(inv, low)]
        inv = [x - dot3(y, x) for x, y in zip(inv, mid)]
        b *= 2
    return inv


def local_kernel(
    xn_ref, w_ref, taps_ref, beta_ref, gc_ref, decay_ref,
    ab_ref, k_ref, uw_ref,
    w_scr, k_scr, v_scr,
):
    length, width = k_ref.shape
    gather_two(w_ref, w_scr)
    raw = dot(xn_ref[...], w_scr[...])
    keys = unit_rows(short_conv(raw[:, :width], taps_ref[0], length, k_scr))
    values = short_conv(raw[:, width:], taps_ref[1], length, v_scr)
    k_ref[...] = keys
    beta = beta_ref[...]
    gc = gc_ref[...]
    kb = keys * beta
    r = lax.broadcasted_iota(jnp.int32, (length, length), 0)
    c = lax.broadcasted_iota(jnp.int32, (length, length), 1)
    corr = jnp.where(r > c, dot3(kb, keys, ((1,), (1,))) * decay_ref[...], 0.0)
    half = length // 2
    first, second = inverse_unit_lower(
        [corr[:half, :half], corr[half:, half:]], half
    )
    rhs = jnp.concatenate([values * beta, kb * jnp.exp(gc)], axis=1)
    top = dot3(first, rhs[:half])
    bottom = dot3(second, rhs[half:] - dot3(corr[half:, :half], top))
    uw_ref[0:half] = top
    uw_ref[half:] = bottom
    last = gc[length - 1 : length, :]
    kd = keys * jnp.exp(last - gc)
    made = dot3(kd, uw_ref[...], ((0,), (0,)))
    ri = lax.broadcasted_iota(jnp.int32, (width, width), 0)
    ci = lax.broadcasted_iota(jnp.int32, (width, width), 1)
    linear = jnp.where(ri == ci, jnp.exp(last), 0.0) - made[:, width:]
    ab_ref[:, :width] = linear.astype(BF16)
    ab_ref[:, width:] = made[:, :width].astype(BF16)


def query_kernel(
    xn_ref, w_ref, taps_ref, gc_ref, decay_ref, k_ref, uw_ref,
    own_ref, eff_ref, silu_ref,
    w_scr, q_scr,
):
    length, width = k_ref.shape
    gather_two(w_ref, w_scr)
    raw = dot(xn_ref[...], w_scr[...])
    query = unit_rows(short_conv(raw[:, :width], taps_ref[0], length, q_scr)) * width ** (-0.5)
    silu_ref[...] = jax.nn.silu(raw[HALO:, width:].astype(BF16).astype(F32))
    scores = dot3(query, k_ref[...], ((1,), (1,))) * decay_ref[...]
    both = dot3(scores, uw_ref[...])
    own_ref[...] = both[:, :width]
    eff_ref[...] = query * jnp.exp(gc_ref[...]) - both[:, width:]


def pool_kernel(
    ids_ref, xn_ref, w_ref, mix_ref, scale_ref, out_ref, wo_ref, w_scr, a_scr, b_scr
):
    _, count, part, width = w_ref.shape
    length = xn_ref.shape[0] - HALO
    for s in range(count):
        at = s * width
        w_scr[at : at + 96, :] = w_ref[0, s]
        w_scr[at + 96 : at + 128, :] = w_ref[1, s, 0:32]
        wo_ref[0:64, at : at + width] = w_ref[1, s, 32:96]
        wo_ref[64:128, at : at + width] = w_ref[2, s, 0:64]
        wo_ref[128:160, at : at + width] = w_ref[2, s, 64:96]
        wo_ref[160:256, at : at + width] = w_ref[3, s]
    x = dot(xn_ref[...], w_scr[...]).astype(BF16).astype(F32)
    kind = ids_ref[1] % 4
    total = HALO + length
    a_scr[0:HALO] = jnp.zeros((HALO, width), F32)
    b_scr[0:HALO] = jnp.zeros((HALO, width), F32)
    a_scr[HALO:] = x
    two = x + a_scr[HALO - 1 : HALO - 1 + total]
    b_scr[HALO:] = two
    four = two + b_scr[HALO - 2 : HALO - 2 + total]
    a_scr[HALO:] = four
    eight = four + a_scr[HALO - 4 : HALO - 4 + total]
    b_scr[HALO:] = eight
    sixteen = eight + b_scr[HALO - 8 : HALO - 8 + total]
    window = jnp.where(kind == 0, two, jnp.where(kind == 1, four, jnp.where(kind == 2, eight, sixteen)))
    window = window[HALO:]
    place = ids_ref[0] * length + lax.broadcasted_iota(jnp.int32, (length, width), 0)
    span = jnp.where(kind == 0, 2, jnp.where(kind == 1, 4, jnp.where(kind == 2, 8, 16)))
    counts = jnp.minimum(place + 1, span).astype(F32)
    pooled = (window / counts - x[HALO:]).astype(BF16)
    out_ref[...] = (dot(pooled, mix_ref[...]) * scale_ref[...]).astype(BF16)


def step_map(later, carry, width):
    ch, cl = split(carry)
    linear = later[:, :width]
    moved = dot(linear, ch) + dot(linear, cl)
    offset = later[:, width:].astype(F32)
    return jnp.concatenate([moved[:, :width], moved[:, width:] + offset], axis=1)


def group_kernel(ids_ref, maps_ref, total_ref, before_ref):
    count, width, _ = maps_ref.shape
    place = ids_ref[0] % count
    r = lax.broadcasted_iota(jnp.int32, (width, width), 0)
    c = lax.broadcasted_iota(jnp.int32, (width, width), 1)
    eye = jnp.where(r == c, 1.0, 0.0)
    carry = jnp.concatenate([eye, jnp.zeros((width, width), F32)], axis=1)
    before = carry
    carry = maps_ref[0].astype(F32)
    for i in range(1, count):
        before = jnp.where(place == i, carry, before)
        carry = step_map(maps_ref[i], carry, width)
    before_ref[...] = before
    total_ref[...] = carry.astype(BF16)


def final_kernel(
    ids_ref, maps_ref, before_ref, own_ref, eff_ref, silu_ref, gain_ref, pool_ref, wo_ref, out_ref
):
    count, width, _ = maps_ref.shape
    group = ids_ref[0] // count
    state = jnp.where(group > 0, maps_ref[0, :, width:].astype(F32), 0.0)
    for i in range(1, count - 1):
        sh, sl = split(state)
        linear = maps_ref[i, :, :width]
        later = dot(linear, sh) + dot(linear, sl) + maps_ref[i, :, width:].astype(F32)
        state = jnp.where(group > i, later, state)
    state = dot3(before_ref[:, :width], state) + before_ref[:, width:]
    attended = own_ref[...] + dot3(eff_ref[...], state)
    scale = lax.rsqrt(jnp.mean(attended * attended, axis=-1, keepdims=True) + EPS)
    delta = (attended * scale * gain_ref[...] * silu_ref[...]).astype(BF16)
    both = jnp.concatenate([pool_ref[...], delta], axis=1)
    groups, rows, cols = out_ref.shape
    step = 512
    for at in range(0, cols, step):
        part = dot(both, wo_ref[:, at : at + step]).astype(BF16)
        for j in range(groups):
            out_ref[j, :, at : at + step] = part[j * rows : (j + 1) * rows]


def sum_kernel(in_ref, out_ref):
    total = in_ref[0].astype(F32)
    for j in range(1, in_ref.shape[0]):
        total = total + in_ref[j].astype(F32)
    out_ref[...] = total.astype(BF16)


def per_device(
    tokens,
    norm_gain,
    w_pool_in,
    w_query,
    w_key,
    w_value,
    w_gate,
    w_beta,
    w_decay,
    conv_weight,
    a_log,
    decay_extra,
    w_mix,
    pool_scale,
    delta_gain,
    w_out_pool,
    w_out_delta,
):
    n_sp = lax.axis_size("sp")
    n_tp = lax.axis_size("tp")
    sp_id = lax.axis_index("sp").astype(jnp.int32)
    tp_id = lax.axis_index("tp").astype(jnp.int32)
    fs_id = lax.axis_index("fs").astype(jnp.int32)
    ids = jnp.stack([sp_id, tp_id])
    f = fs_id[None]
    depth, width = w_key.shape
    rows, model = tokens.shape
    length = rows * n_tp
    half = depth // 2

    kv_copies = call(pack_first, shape(n_sp, half, width, dtype=BF16), f, w_key, w_value, smem=1)
    kv_part = exchange(kv_copies, "sp")
    all_rows = exchange(everyone(tokens, "tp"), "tp").reshape(length, model)
    qg_copies, poo_copies = call(
        pack_rest,
        (shape(n_sp, half, width, dtype=BF16), shape(n_sp, 3 * depth // 4, width, dtype=BF16)),
        f, w_query, w_gate, w_pool_in, w_out_pool, w_out_delta,
        smem=1, scratch=[pltpu.VMEM((3 * depth, width), BF16)],
    )
    tail = lax.ppermute(
        all_rows[length - HALO :], "sp", [(i, i + 1) for i in range(n_sp - 1)]
    )
    kv = exchange(everyone(kv_part, "fs"), "fs").reshape(4, n_sp, half, width)
    qg_copies, poo_copies, _ = lax.optimization_barrier((qg_copies, poo_copies, kv_part))
    qg_part = exchange(qg_copies, "sp")
    qg = exchange(everyone(qg_part, "fs"), "fs").reshape(4, n_sp, half, width)
    poo_part = exchange(poo_copies, "sp")
    poo = exchange(everyone(poo_part, "fs"), "fs").reshape(4, n_sp, 3 * depth // 4, width)

    wbd = jnp.concatenate([w_beta.T, w_decay.T], axis=0)
    xn, beta, gc, decay = call(
        norm_kernel,
        (
            shape(HALO + length, model, dtype=BF16),
            shape(length, 128),
            shape(length, 128),
            shape(length, length),
        ),
        ids, a_log, all_rows, tail, norm_gain.reshape(1, model), wbd, decay_extra,
        smem=2, flops=2 * length * model * 128,
    )
    ab, keys, uw = call(
        local_kernel,
        (shape(width, 2 * width, dtype=BF16), shape(length, width), shape(length, 2 * width)),
        xn, kv, conv_weight[1:], beta, gc, decay,
        scratch=[
            pltpu.VMEM((model, 2 * width), BF16),
            pltpu.VMEM((HALO + length, width), F32),
            pltpu.VMEM((HALO + length, width), F32),
        ],
        flops=20 * length * model * width,
    )
    quad = 4
    near = [[quad * g + r for r in range(quad)] for g in range(n_sp // quad)]
    far = [[quad * g + r for g in range(n_sp // quad)] for r in range(quad)]
    near_maps = exchange(jnp.broadcast_to(ab, (quad, *ab.shape)), "sp", near)
    total, before = call(
        group_kernel,
        (shape(width, 2 * width, dtype=BF16), shape(width, 2 * width)),
        ids, near_maps,
        smem=1, flops=20 * width**3,
    )
    far_maps = lax.all_gather(total, "sp", axis=0, axis_index_groups=far)

    own, eff, silu_gate = call(
        query_kernel,
        (shape(length, width), shape(length, width), shape(length, width)),
        xn, qg, conv_weight[:1], gc, decay, keys, uw,
        scratch=[
            pltpu.VMEM((model, 2 * width), BF16),
            pltpu.VMEM((HALO + length, width), F32),
        ],
        flops=8 * length * model * width,
    )
    pool_out, w_out = call(
        pool_kernel,
        (shape(length, width, dtype=BF16), shape(2 * width, model, dtype=BF16)),
        ids, xn, poo, w_mix[0], pool_scale.reshape(1, width),
        smem=1,
        scratch=[
            pltpu.VMEM((model, width), BF16),
            pltpu.VMEM((2 * HALO + length, width), F32),
            pltpu.VMEM((2 * HALO + length, width), F32),
        ],
        flops=4 * length * model * width,
    )
    partial = call(
        final_kernel,
        shape(n_tp, rows, model, dtype=BF16),
        ids, far_maps, before, own, eff, silu_gate, delta_gain.reshape(1, width), pool_out, w_out,
        smem=1, flops=4 * length * model * width,
    )
    arrived = exchange(partial, "tp")
    return call(sum_kernel, shape(rows, model, dtype=BF16), arrived, flops=1000000)


def solution(mesh):
    placed = (
        P(("fs", "sp", "tp"), None),
        P(),
        P("sp", "tp"),
        P("sp", "tp"),
        P("sp", "tp"),
        P("sp", "tp"),
        P("sp", "tp"),
        P(),
        P(),
        P(None, None, "tp"),
        P("tp"),
        P(("fs", "sp"), "tp"),
        P("tp", None, None),
        P("tp"),
        P(),
        P("tp", "sp"),
        P("tp", "sp"),
    )
    return jax.shard_map(
        per_device,
        mesh=mesh,
        in_specs=placed,
        out_specs=P(("fs", "sp", "tp"), None),
        check_vma=False,
    )
```

```python
import jax
import jax.numpy as jnp
from jax import lax
from jax.experimental import pallas as pl
from jax.experimental.pallas import tpu as pltpu
from jax.sharding import PartitionSpec as P


EPS = 1e-06
HALO = 16
F32 = jnp.float32
BF16 = jnp.bfloat16


def call(kernel, outs, *args, smem=0, scratch=(), flops=0, vmem=16):
    in_specs = [pl.BlockSpec(memory_space=pltpu.SMEM)] * smem + [
        pl.BlockSpec(memory_space=pltpu.VMEM)
    ] * (len(args) - smem)
    many = isinstance(outs, (list, tuple))
    out_specs = pl.BlockSpec(memory_space=pltpu.VMEM)
    return pl.pallas_call(
        kernel,
        out_shape=list(outs) if many else outs,
        in_specs=in_specs,
        out_specs=[out_specs] * len(outs) if many else out_specs,
        scratch_shapes=list(scratch),
        compiler_params=pltpu.CompilerParams(vmem_limit_bytes=vmem and vmem * 1024 * 1024),
        cost_estimate=pl.CostEstimate(flops=flops, bytes_accessed=0, transcendentals=0),
    )(*args)


def shape(*dims, dtype=F32):
    return jax.ShapeDtypeStruct(dims, dtype)


def dot(a, b, dims=((1,), (0,))):
    return lax.dot_general(a, b, (dims, ((), ())), preferred_element_type=F32)


def split(a):
    high = a.astype(BF16)
    return high, (a - high.astype(F32)).astype(BF16)


def dot3(a, b, dims=((1,), (0,))):
    ah, al = split(a)
    bh, bl = split(b)
    return dot(ah, bh, dims) + (dot(ah, bl, dims) + dot(al, bh, dims))


def start_kernel(
    f_ref, tok_ref, gain_ref, k_ref, v_ref, q_ref, g_ref, p_ref, op_ref, od_ref,
    copies_ref, part_ref, stacked,
):
    x = tok_ref[...].astype(F32)
    scale = lax.rsqrt(jnp.mean(x * x, axis=-1, keepdims=True) + EPS)
    normed = (x * scale * gain_ref[...].astype(F32)).astype(BF16)
    for j in range(copies_ref.shape[0]):
        copies_ref[j] = normed
    f = f_ref[0]
    depth = k_ref.shape[0]
    half = depth // 2
    rows = pl.ds(pl.multiple_of((f % 2) * half, half), half)
    part_ref[0:half] = jnp.where(f < 2, k_ref[rows, :], v_ref[rows, :])
    part_ref[half:depth] = jnp.where(f < 2, q_ref[rows, :], g_ref[rows, :])
    stacked[0:depth] = p_ref[...]
    stacked[depth : 2 * depth] = op_ref[...]
    stacked[2 * depth :] = od_ref[...]
    third = 3 * depth // 4
    part_ref[depth:] = stacked[pl.ds(pl.multiple_of(f * third, 32), third), :]


def exchange(copies, axis, groups=None):
    return lax.all_to_all(
        copies, axis, split_axis=0, concat_axis=0, tiled=True, axis_index_groups=groups
    )


def turns(x, axis, size):
    n = lax.axis_size(axis)
    out = [x]
    for d in range(1, size):
        out.append(lax.ppermute(x, axis, [(i, i - i % size + (i + d) % size) for i in range(n)]))
    return out


def gate_kernel(
    ids_ref, a_log_ref, rows_ref, tail_ref, wbd_ref, extra_ref, xn_ref, beta_ref, gc_ref, decay_ref
):
    length = rows_ref.shape[0]
    tail = tail_ref[...]
    xn_ref[0:HALO] = jnp.where(ids_ref[0] > 0, tail, jnp.zeros_like(tail))
    xn_ref[HALO:] = rows_ref[...]
    pre = dot(rows_ref[...], wbd_ref[...], ((1,), (1,)))
    heads = pre.shape[1] // 2
    col = lax.broadcasted_iota(jnp.int32, pre.shape, 1)
    lane = ids_ref[1]
    beta_pre = jnp.sum(jnp.where(col == lane, pre, 0.0), axis=1, keepdims=True)
    decay_pre = jnp.sum(jnp.where(col == lane + heads, pre, 0.0), axis=1, keepdims=True)
    wide = (length, 128)
    beta_ref[...] = jax.nn.sigmoid(jnp.broadcast_to(beta_pre, wide))
    rate = jnp.exp(jnp.full(wide, a_log_ref[0], F32))
    soft = jax.nn.softplus(jnp.broadcast_to(decay_pre, wide))
    log_gate = -rate * soft + jnp.broadcast_to(extra_ref[...], wide)
    r = lax.broadcasted_iota(jnp.int32, (length, length), 0)
    c = lax.broadcasted_iota(jnp.int32, (length, length), 1)
    lower = jnp.where(r >= c, 1.0, 0.0).astype(BF16)
    g1 = log_gate.astype(BF16)
    rest = log_gate - g1.astype(F32)
    g2 = rest.astype(BF16)
    g3 = (rest - g2.astype(F32)).astype(BF16)
    gc = dot(lower, g1) + (dot(lower, g2) + dot(lower, g3))
    gc_ref[...] = gc
    across = jnp.transpose(gc)
    across = jnp.concatenate([across] * (length // 128), axis=0)
    along = jnp.concatenate([gc] * (length // 128), axis=1)
    gaps = along - across
    decay_ref[...] = jnp.where(r >= c, jnp.exp(jnp.where(r >= c, gaps, 0.0)), 0.0)


def gather_two(f, pieces, w_scr):
    count, _, width = pieces[0].shape
    half = width // 2
    for d, piece in enumerate(pieces):
        slot = (f + 4 - d) % 4
        cols = pl.ds(pl.multiple_of((slot // 2) * width, width), width)
        for s in range(count):
            at = pl.multiple_of((2 * s + slot % 2) * half, half)
            w_scr[pl.ds(at, half), cols] = piece[s, 0:half]


def short_conv(raw, taps, length, x_scr):
    x_scr[...] = raw.astype(BF16).astype(F32)
    conv = jnp.zeros((length, raw.shape[1]), F32)
    for j in range(4):
        conv = conv + x_scr[HALO - 3 + j : HALO - 3 + j + length, :] * taps[j : j + 1, :]
    return jax.nn.silu(conv)


def unit_rows(x):
    return x * lax.rsqrt(jnp.sum(x * x, axis=-1, keepdims=True) + EPS)


def inverse_unit_lower(low, size):
    r = lax.broadcasted_iota(jnp.int32, (size, size), 0)
    c = lax.broadcasted_iota(jnp.int32, (size, size), 1)
    inv = [jnp.where(r == c, 1.0, 0.0) - jnp.where((r // 2 == c // 2) & (r > c), x, 0.0) for x in low]
    b = 2
    while b < size:
        mask = (r // (2 * b) == c // (2 * b)) & (r % (2 * b) >= b) & (c % (2 * b) < b)
        mid = [dot3(x, jnp.where(mask, y, 0.0)) for x, y in zip(inv, low)]
        inv = [x - dot3(y, x) for x, y in zip(inv, mid)]
        b *= 2
    return inv


def local_kernel(
    xn_ref, w_ref, taps_ref, beta_ref, gc_ref, decay_ref,
    ab_ref, k_ref, uw_ref,
    w_scr, k_scr, v_scr,
):
    length, width = k_ref.shape
    count, half = w_ref.shape[1:3]
    for m in range(2):
        for h in range(2):
            for i in range(count):
                at = (2 * i + h) * half
                w_scr[at : at + half, m * width : (m + 1) * width] = w_ref[2 * m + h, i]
    raw = dot(xn_ref[...], w_scr[...])
    keys = unit_rows(short_conv(raw[:, :width], taps_ref[0], length, k_scr))
    values = short_conv(raw[:, width:], taps_ref[1], length, v_scr)
    k_ref[...] = keys
    beta = beta_ref[...]
    gc = gc_ref[...]
    kb = keys * beta
    r = lax.broadcasted_iota(jnp.int32, (length, length), 0)
    c = lax.broadcasted_iota(jnp.int32, (length, length), 1)
    corr = jnp.where(r > c, dot3(kb, keys, ((1,), (1,))) * decay_ref[...], 0.0)
    half = length // 2
    first, second = inverse_unit_lower(
        [corr[:half, :half], corr[half:, half:]], half
    )
    rhs = jnp.concatenate([values * beta, kb * jnp.exp(gc)], axis=1)
    top = dot3(first, rhs[:half])
    bottom = dot3(second, rhs[half:] - dot3(corr[half:, :half], top))
    uw_ref[0:half] = top
    uw_ref[half:] = bottom
    last = gc[length - 1 : length, :]
    kd = keys * jnp.exp(last - gc)
    made = dot3(kd, uw_ref[...], ((0,), (0,)))
    ri = lax.broadcasted_iota(jnp.int32, (width, width), 0)
    ci = lax.broadcasted_iota(jnp.int32, (width, width), 1)
    linear = jnp.where(ri == ci, jnp.exp(last), 0.0) - made[:, width:]
    ab_ref[:, :width] = linear.astype(BF16)
    ab_ref[:, width:] = made[:, :width].astype(BF16)


def query_kernel(
    ids_ref, xn_ref, w0_ref, w1_ref, w2_ref, w3_ref, taps_ref, gc_ref, decay_ref, k_ref, uw_ref,
    own_ref, eff_ref, silu_ref,
    w_scr, q_scr,
):
    length, width = k_ref.shape
    gather_two(ids_ref[2], (w0_ref, w1_ref, w2_ref, w3_ref), w_scr)
    raw = dot(xn_ref[...], w_scr[...])
    query = unit_rows(short_conv(raw[:, :width], taps_ref[0], length, q_scr)) * width ** (-0.5)
    silu_ref[...] = jax.nn.silu(raw[HALO:, width:].astype(BF16).astype(F32))
    scores = dot3(query, k_ref[...], ((1,), (1,))) * decay_ref[...]
    both = dot3(scores, uw_ref[...])
    own_ref[...] = both[:, :width]
    eff_ref[...] = query * jnp.exp(gc_ref[...]) - both[:, width:]


def pool_kernel(
    ids_ref, xn_ref, w0_ref, w1_ref, w2_ref, w3_ref, mix_ref, scale_ref,
    out_ref, wo_ref, w_all, w_scr, a_scr, b_scr,
):
    count, part, width = w0_ref.shape
    skip = width // 2
    part = part - skip
    length = xn_ref.shape[0] - HALO
    for d, piece in enumerate((w0_ref, w1_ref, w2_ref, w3_ref)):
        at = pl.multiple_of(((ids_ref[2] + 4 - d) % 4) * part, 32)
        for s in range(count):
            w_all[pl.ds(at, part), s * width : (s + 1) * width] = piece[s, skip:]
    for s in range(count):
        w_scr[s * width : (s + 1) * width, :] = w_all[0:width, s * width : (s + 1) * width]
    wo_ref[...] = w_all[width:, :]
    x = dot(xn_ref[...], w_scr[...]).astype(BF16).astype(F32)
    kind = ids_ref[1] % 4
    total = HALO + length
    a_scr[0:HALO] = jnp.zeros((HALO, width), F32)
    b_scr[0:HALO] = jnp.zeros((HALO, width), F32)
    a_scr[HALO:] = x
    two = x + a_scr[HALO - 1 : HALO - 1 + total]
    b_scr[HALO:] = two
    four = two + b_scr[HALO - 2 : HALO - 2 + total]
    a_scr[HALO:] = four
    eight = four + a_scr[HALO - 4 : HALO - 4 + total]
    b_scr[HALO:] = eight
    sixteen = eight + b_scr[HALO - 8 : HALO - 8 + total]
    window = jnp.where(kind == 0, two, jnp.where(kind == 1, four, jnp.where(kind == 2, eight, sixteen)))
    window = window[HALO:]
    place = ids_ref[0] * length + lax.broadcasted_iota(jnp.int32, (length, width), 0)
    span = jnp.where(kind == 0, 2, jnp.where(kind == 1, 4, jnp.where(kind == 2, 8, 16)))
    counts = jnp.minimum(place + 1, span).astype(F32)
    pooled = (window / counts - x[HALO:]).astype(BF16)
    out_ref[...] = (dot(pooled, mix_ref[...]) * scale_ref[...]).astype(BF16)


def step_map(later, carry, width):
    ch, cl = split(carry)
    linear = later[:, :width]
    moved = dot(linear, ch) + dot(linear, cl)
    offset = later[:, width:].astype(F32)
    return jnp.concatenate([moved[:, :width], moved[:, width:] + offset], axis=1)


def group_kernel(
    ids_ref, m0_ref, m1_ref, m2_ref, m3_ref, total_ref, linear_ref, offset_ref, before_ref, maps
):
    count, width, _ = maps.shape
    place = ids_ref[0] % count
    for d, piece in enumerate((m0_ref, m1_ref, m2_ref, m3_ref)):
        maps[(place + count - d) % count] = piece[...]
    r = lax.broadcasted_iota(jnp.int32, (width, width), 0)
    c = lax.broadcasted_iota(jnp.int32, (width, width), 1)
    eye = jnp.where(r == c, 1.0, 0.0)
    before = jnp.concatenate([eye, jnp.zeros((width, width), F32)], axis=1)
    carry = maps[0].astype(F32)
    for i in range(1, count):
        before = jnp.where(place == i, carry, before)
        carry = step_map(maps[i], carry, width)
    before_ref[...] = before
    total = carry.astype(BF16)
    total_ref[...] = total
    linear_ref[...] = total[:, :width]
    offset_ref[...] = total[:, width:]


def apply(linear, state):
    high, low = split(state)
    return dot(linear, high) + dot(linear, low)


def attend_kernel(
    ids_ref, t4_ref, a8_ref, b8_ref, b12_ref, before_ref, own_ref, eff_ref, silu_ref, gain_ref,
    pool_ref, mine_ref, other_ref,
):
    width = b8_ref.shape[0]
    state = apply(a8_ref[...], b12_ref[...].astype(F32)) + b8_ref[...].astype(F32)
    state = apply(t4_ref[:, :width], state) + t4_ref[:, width:].astype(F32)
    state = dot3(before_ref[:, :width], state) + before_ref[:, width:]
    attended = own_ref[...] + dot3(eff_ref[...], state)
    scale = lax.rsqrt(jnp.mean(attended * attended, axis=-1, keepdims=True) + EPS)
    delta = (attended * scale * gain_ref[...] * silu_ref[...]).astype(BF16)
    both = jnp.concatenate([pool_ref[...], delta], axis=1)
    core = ids_ref[1] % 2
    chips, rows = mine_ref.shape[:2]
    for j in range(chips):
        even = both[2 * j * rows : (2 * j + 1) * rows]
        odd = both[(2 * j + 1) * rows : (2 * j + 2) * rows]
        mine_ref[j] = jnp.where(core == 0, even, odd)
        other_ref[j] = jnp.where(core == 0, odd, even)


def out_kernel(mine_ref, theirs_ref, w_mine_ref, w_theirs_ref, out_ref):
    chips, rows, width = mine_ref.shape
    mine = mine_ref[...].reshape(chips * rows, width)
    theirs = theirs_ref[...].reshape(chips * rows, width)
    cols = out_ref.shape[2]
    step = 512
    for at in range(0, cols, step):
        part = dot(mine, w_mine_ref[:, at : at + step]) + dot(theirs, w_theirs_ref[:, at : at + step])
        out_ref[:, :, at : at + step] = part.astype(BF16).reshape(chips, rows, step)


def sum_kernel(in_ref, out_ref):
    total = in_ref[0].astype(F32)
    for j in range(1, in_ref.shape[0]):
        total = total + in_ref[j].astype(F32)
    out_ref[...] = total.astype(BF16)


def layer(
    tokens,
    norm_gain,
    w_pool_in,
    w_query,
    w_key,
    w_value,
    w_gate,
    w_beta,
    w_decay,
    conv_weight,
    a_log,
    decay_extra,
    w_mix,
    pool_scale,
    delta_gain,
    w_out_pool,
    w_out_delta,
):
    n_sp = lax.axis_size("sp")
    n_tp = lax.axis_size("tp")
    sp_id = lax.axis_index("sp").astype(jnp.int32)
    tp_id = lax.axis_index("tp").astype(jnp.int32)
    fs_id = lax.axis_index("fs").astype(jnp.int32)
    ids = jnp.stack([sp_id, tp_id, fs_id])
    depth, width = w_key.shape
    rows, model = tokens.shape
    length = rows * n_tp
    half = depth // 2

    copies, part = call(
        start_kernel,
        (shape(n_tp, rows, model, dtype=BF16), shape(7 * depth // 4, width, dtype=BF16)),
        fs_id[None], tokens, norm_gain.reshape(1, model),
        w_key, w_value, w_query, w_gate, w_pool_in, w_out_pool, w_out_delta,
        smem=1, scratch=[pltpu.VMEM((3 * depth, width), BF16)], vmem=None,
    )
    all_rows = exchange(copies, "tp").reshape(length, model)
    tail = lax.ppermute(
        all_rows[length - HALO :], "sp", [(i, i + 1) for i in range(n_sp - 1)]
    )
    quarters = lax.all_gather(part, "sp", axis=0)
    kv = exchange(
        jnp.broadcast_to(quarters[:, :half], (4, n_sp, half, width)), "fs"
    )
    kv = kv.reshape(4, n_sp, half, width)
    rest = turns(quarters[:, half:], "fs", 4)

    wbd = jnp.concatenate([w_beta.T, w_decay.T], axis=0)
    xn, beta, gc, decay = call(
        gate_kernel,
        (
            shape(HALO + length, model, dtype=BF16),
            shape(length, 128),
            shape(length, 128),
            shape(length, length),
        ),
        ids, a_log, all_rows, tail, wbd, decay_extra,
        smem=2, flops=2 * length * model * 128,
    )
    ab, keys, uw = call(
        local_kernel,
        (shape(width, 2 * width, dtype=BF16), shape(length, width), shape(length, 2 * width)),
        xn, kv, conv_weight[1:], beta, gc, decay,
        scratch=[
            pltpu.VMEM((model, 2 * width), BF16),
            pltpu.VMEM((HALO + length, width), F32),
            pltpu.VMEM((HALO + length, width), F32),
        ],
        flops=20 * length * model * width,
    )
    quad = 4
    near = turns(ab, "sp", quad)
    total, linear, offset, before = call(
        group_kernel,
        (
            shape(width, 2 * width, dtype=BF16),
            shape(width, width, dtype=BF16),
            shape(width, width, dtype=BF16),
            shape(width, 2 * width),
        ),
        ids, *near,
        smem=1, scratch=[pltpu.VMEM((quad, width, 2 * width), BF16)], flops=20 * width**3,
    )

    def from_behind(x, first, last, distance):
        return lax.ppermute(x, "sp", [(i, i + distance) for i in range(first, last)])

    t4 = from_behind(total, 0, n_sp - quad, quad)
    b8 = from_behind(offset, 0, n_sp - 2 * quad, 2 * quad)
    a8 = from_behind(linear, quad, n_sp - 2 * quad, 2 * quad)
    b12 = from_behind(offset, 0, n_sp - 3 * quad, 3 * quad)

    own, eff, silu_gate = call(
        query_kernel,
        (shape(length, width), shape(length, width), shape(length, width)),
        ids, xn, *rest, conv_weight[:1], gc, decay, keys, uw,
        smem=1,
        scratch=[
            pltpu.VMEM((model, 2 * width), BF16),
            pltpu.VMEM((HALO + length, width), F32),
        ],
        flops=8 * length * model * width,
    )
    pool_out, w_mine = call(
        pool_kernel,
        (shape(length, width, dtype=BF16), shape(2 * width, model, dtype=BF16)),
        ids, xn, *rest, w_mix[0], pool_scale.reshape(1, width),
        smem=1,
        scratch=[
            pltpu.VMEM((3 * width, model), BF16),
            pltpu.VMEM((model, width), BF16),
            pltpu.VMEM((2 * HALO + length, width), F32),
            pltpu.VMEM((2 * HALO + length, width), F32),
        ],
        flops=8 * length * model * width,
    )
    swap = [(i, i ^ 1) for i in range(n_tp)]
    w_theirs = lax.ppermute(w_mine, "tp", swap)
    chips = n_tp // 2
    mine, other = call(
        attend_kernel,
        (shape(chips, rows, 2 * width, dtype=BF16), shape(chips, rows, 2 * width, dtype=BF16)),
        ids, t4, a8, b8, b12, before, own, eff, silu_gate, delta_gain.reshape(1, width), pool_out,
        smem=1, flops=4 * length * model * width,
    )
    theirs = lax.ppermute(other, "tp", swap)
    partial = call(
        out_kernel,
        shape(chips, rows, model, dtype=BF16),
        mine, theirs, w_mine, w_theirs,
        flops=4 * length * model * width,
    )
    cores = [[2 * x + c for x in range(chips)] for c in range(2)]
    arrived = exchange(partial, "tp", cores)
    return call(sum_kernel, shape(rows, model, dtype=BF16), arrived, flops=1000000)


def solution(mesh):
    placed = (
        P(("fs", "sp", "tp"), None),
        P(),
        P("sp", "tp"),
        P("sp", "tp"),
        P("sp", "tp"),
        P("sp", "tp"),
        P("sp", "tp"),
        P(),
        P(),
        P(None, None, "tp"),
        P("tp"),
        P(("fs", "sp"), "tp"),
        P("tp", None, None),
        P("tp"),
        P(),
        P("tp", "sp"),
        P("tp", "sp"),
    )
    return jax.shard_map(
        layer,
        mesh=mesh,
        in_specs=placed,
        out_specs=P(("fs", "sp", "tp"), None),
        check_vma=False,
    )
```

```python
import jax
import jax.numpy as jnp
from jax import lax
from jax.experimental import pallas as pl
from jax.experimental.pallas import tpu as pltpu
from jax.sharding import PartitionSpec as P


EPS = 1e-06
HALO = 16
F32 = jnp.float32
BF16 = jnp.bfloat16


def call(kernel, outs, *args, smem=3, scratch=(), flops=0, vmem=16):
    in_specs = [pl.BlockSpec(memory_space=pltpu.SMEM)] * smem + [
        pl.BlockSpec(memory_space=pltpu.VMEM)
    ] * (len(args) - smem)
    many = isinstance(outs, (list, tuple))
    out_specs = pl.BlockSpec(memory_space=pltpu.VMEM)
    return pl.pallas_call(
        kernel,
        out_shape=list(outs) if many else outs,
        in_specs=in_specs,
        out_specs=[out_specs] * len(outs) if many else out_specs,
        scratch_shapes=list(scratch),
        compiler_params=pltpu.CompilerParams(vmem_limit_bytes=vmem and vmem * 1024 * 1024),
        cost_estimate=pl.CostEstimate(flops=flops, bytes_accessed=0, transcendentals=0),
    )(*args)


def shape(*dims, dtype=F32):
    return jax.ShapeDtypeStruct(dims, dtype)


def dot(a, b, dims=((1,), (0,))):
    return lax.dot_general(a, b, (dims, ((), ())), preferred_element_type=F32)


def split(a):
    high = a.astype(BF16)
    return high, (a - high.astype(F32)).astype(BF16)


def dot3(a, b, dims=((1,), (0,))):
    ah, al = split(a)
    bh, bl = split(b)
    return dot(ah, bh, dims) + (dot(ah, bl, dims) + dot(al, bh, dims))


def start_kernel(
    sp_ref, tp_ref, fs_ref, tok_ref, gain_ref, k_ref, v_ref, q_ref, g_ref, p_ref, op_ref, od_ref,
    copies_ref, part_ref, stacked,
):
    x = tok_ref[...].astype(F32)
    scale = lax.rsqrt(jnp.mean(x * x, axis=-1, keepdims=True) + EPS)
    gain = gain_ref[...].astype(F32).reshape(1, x.shape[1])
    normed = (x * scale * gain).astype(BF16)
    for j in range(copies_ref.shape[0]):
        copies_ref[j] = normed
    f = fs_ref[0]
    depth = k_ref.shape[0]
    half = depth // 2
    rows = pl.ds(pl.multiple_of((f % 2) * half, half), half)
    part_ref[0:half] = jnp.where(f < 2, k_ref[rows, :], v_ref[rows, :])
    part_ref[half:depth] = jnp.where(f < 2, q_ref[rows, :], g_ref[rows, :])
    stacked[0:depth] = p_ref[...]
    stacked[depth : 2 * depth] = op_ref[...]
    stacked[2 * depth :] = od_ref[...]
    third = 3 * depth // 4
    part_ref[depth:] = stacked[pl.ds(pl.multiple_of(f * third, 32), third), :]


def exchange(copies, axis, groups=None):
    return lax.all_to_all(
        copies, axis, split_axis=0, concat_axis=0, tiled=True, axis_index_groups=groups
    )


def turns(x, axis, size):
    n = lax.axis_size(axis)
    out = [x]
    for d in range(1, size):
        out.append(lax.ppermute(x, axis, [(i, i - i % size + (i + d) % size) for i in range(n)]))
    return out


def gate_kernel(
    sp_ref, tp_ref, fs_ref, a_log_ref, rows_ref, tail_ref, wb_ref, wd_ref, extra_ref,
    xn_ref, beta_ref, gc_ref, decay_ref,
):
    length = rows_ref.shape[0]
    tail = tail_ref[...]
    xn_ref[0:HALO] = jnp.where(sp_ref[0] > 0, tail, jnp.zeros_like(tail))
    xn_ref[HALO:] = rows_ref[...]
    lane = tp_ref[0]

    def own_column(w_ref):
        pre = dot(rows_ref[...], w_ref[...], ((1,), (1,)))
        col = lax.broadcasted_iota(jnp.int32, pre.shape, 1)
        return jnp.sum(jnp.where(col == lane, pre, 0.0), axis=1, keepdims=True)

    beta_pre, decay_pre = own_column(wb_ref), own_column(wd_ref)
    wide = (length, 128)
    beta_ref[...] = jax.nn.sigmoid(jnp.broadcast_to(beta_pre, wide))
    rate = jnp.exp(jnp.full(wide, a_log_ref[0], F32))
    soft = jax.nn.softplus(jnp.broadcast_to(decay_pre, wide))
    extra = jnp.transpose(jnp.broadcast_to(extra_ref[...], (128, length)))
    log_gate = -rate * soft + extra
    r = lax.broadcasted_iota(jnp.int32, (length, length), 0)
    c = lax.broadcasted_iota(jnp.int32, (length, length), 1)
    lower = jnp.where(r >= c, 1.0, 0.0).astype(BF16)
    g1 = log_gate.astype(BF16)
    rest = log_gate - g1.astype(F32)
    g2 = rest.astype(BF16)
    g3 = (rest - g2.astype(F32)).astype(BF16)
    gc = dot(lower, g1) + (dot(lower, g2) + dot(lower, g3))
    gc_ref[...] = gc
    across = jnp.transpose(gc)
    across = jnp.concatenate([across] * (length // 128), axis=0)
    along = jnp.concatenate([gc] * (length // 128), axis=1)
    gaps = along - across
    decay_ref[...] = jnp.where(r >= c, jnp.exp(jnp.where(r >= c, gaps, 0.0)), 0.0)


def gather_two(f, pieces, w_scr):
    count, _, width = pieces[0].shape
    half = width // 2
    for d, piece in enumerate(pieces):
        slot = (f + 4 - d) % 4
        cols = pl.ds(pl.multiple_of((slot // 2) * width, width), width)
        for s in range(count):
            at = pl.multiple_of((2 * s + slot % 2) * half, half)
            w_scr[pl.ds(at, half), cols] = piece[s, 0:half]


def short_conv(raw, taps, length, x_scr):
    x_scr[...] = raw.astype(BF16).astype(F32)
    conv = jnp.zeros((length, raw.shape[1]), F32)
    for j in range(4):
        conv = conv + x_scr[HALO - 3 + j : HALO - 3 + j + length, :] * taps[j : j + 1, :]
    return jax.nn.silu(conv)


def unit_rows(x):
    return x * lax.rsqrt(jnp.sum(x * x, axis=-1, keepdims=True) + EPS)


def inverse_unit_lower(low, size):
    r = lax.broadcasted_iota(jnp.int32, (size, size), 0)
    c = lax.broadcasted_iota(jnp.int32, (size, size), 1)
    inv = [jnp.where(r == c, 1.0, 0.0) - jnp.where((r // 2 == c // 2) & (r > c), x, 0.0) for x in low]
    b = 2
    while b < size:
        mask = (r // (2 * b) == c // (2 * b)) & (r % (2 * b) >= b) & (c % (2 * b) < b)
        mid = [dot3(x, jnp.where(mask, y, 0.0)) for x, y in zip(inv, low)]
        inv = [x - dot3(y, x) for x, y in zip(inv, mid)]
        b *= 2
    return inv


def local_kernel(
    sp_ref, tp_ref, fs_ref, xn_ref, w0_ref, w1_ref, w2_ref, w3_ref, taps_ref, beta_ref, gc_ref, decay_ref,
    ab_ref, k_ref, uw_ref,
    w_scr, k_scr, v_scr,
):
    length, width = k_ref.shape
    gather_two(fs_ref[0], (w0_ref, w1_ref, w2_ref, w3_ref), w_scr)
    raw = dot(xn_ref[...], w_scr[...])
    keys = unit_rows(short_conv(raw[:, :width], taps_ref[1], length, k_scr))
    values = short_conv(raw[:, width:], taps_ref[2], length, v_scr)
    k_ref[...] = keys
    beta = beta_ref[...]
    gc = gc_ref[...]
    kb = keys * beta
    r = lax.broadcasted_iota(jnp.int32, (length, length), 0)
    c = lax.broadcasted_iota(jnp.int32, (length, length), 1)
    corr = jnp.where(r > c, dot3(kb, keys, ((1,), (1,))) * decay_ref[...], 0.0)
    half = length // 2
    first, second = inverse_unit_lower(
        [corr[:half, :half], corr[half:, half:]], half
    )
    rhs = jnp.concatenate([values * beta, kb * jnp.exp(gc)], axis=1)
    top = dot3(first, rhs[:half])
    bottom = dot3(second, rhs[half:] - dot3(corr[half:, :half], top))
    uw_ref[0:half] = top
    uw_ref[half:] = bottom
    last = gc[length - 1 : length, :]
    kd = keys * jnp.exp(last - gc)
    made = dot3(kd, uw_ref[...], ((0,), (0,)))
    ri = lax.broadcasted_iota(jnp.int32, (width, width), 0)
    ci = lax.broadcasted_iota(jnp.int32, (width, width), 1)
    linear = jnp.where(ri == ci, jnp.exp(last), 0.0) - made[:, width:]
    ab_ref[:, :width] = linear.astype(BF16)
    ab_ref[:, width:] = made[:, :width].astype(BF16)


def query_kernel(
    sp_ref, tp_ref, fs_ref, xn_ref, w0_ref, w1_ref, w2_ref, w3_ref, taps_ref, gc_ref, decay_ref, k_ref, uw_ref,
    own_ref, eff_ref, silu_ref,
    w_scr, q_scr,
):
    length, width = k_ref.shape
    gather_two(fs_ref[0], (w0_ref, w1_ref, w2_ref, w3_ref), w_scr)
    raw = dot(xn_ref[...], w_scr[...])
    query = unit_rows(short_conv(raw[:, :width], taps_ref[0], length, q_scr)) * width ** (-0.5)
    silu_ref[...] = jax.nn.silu(raw[HALO:, width:].astype(BF16).astype(F32))
    scores = dot3(query, k_ref[...], ((1,), (1,))) * decay_ref[...]
    both = dot3(scores, uw_ref[...])
    own_ref[...] = both[:, :width]
    eff_ref[...] = query * jnp.exp(gc_ref[...]) - both[:, width:]


def pool_kernel(
    sp_ref, tp_ref, fs_ref, xn_ref, w0_ref, w1_ref, w2_ref, w3_ref, mix_ref, scale_ref,
    out_ref, wo_ref, w_all, w_scr, a_scr, b_scr,
):
    count, part, width = w0_ref.shape
    skip = width // 2
    part = part - skip
    length = xn_ref.shape[0] - HALO
    for d, piece in enumerate((w0_ref, w1_ref, w2_ref, w3_ref)):
        at = pl.multiple_of(((fs_ref[0] + 4 - d) % 4) * part, 32)
        for s in range(count):
            w_all[pl.ds(at, part), s * width : (s + 1) * width] = piece[s, skip:]
    for s in range(count):
        w_scr[s * width : (s + 1) * width, :] = w_all[0:width, s * width : (s + 1) * width]
    wo_ref[...] = w_all[width:, :]
    x = dot(xn_ref[...], w_scr[...]).astype(BF16).astype(F32)
    kind = tp_ref[0] % 4
    total = HALO + length
    a_scr[0:HALO] = jnp.zeros((HALO, width), F32)
    b_scr[0:HALO] = jnp.zeros((HALO, width), F32)
    a_scr[HALO:] = x
    two = x + a_scr[HALO - 1 : HALO - 1 + total]
    b_scr[HALO:] = two
    four = two + b_scr[HALO - 2 : HALO - 2 + total]
    a_scr[HALO:] = four
    eight = four + a_scr[HALO - 4 : HALO - 4 + total]
    b_scr[HALO:] = eight
    sixteen = eight + b_scr[HALO - 8 : HALO - 8 + total]
    window = jnp.where(kind == 0, two, jnp.where(kind == 1, four, jnp.where(kind == 2, eight, sixteen)))
    window = window[HALO:]
    place = sp_ref[0] * length + lax.broadcasted_iota(jnp.int32, (length, width), 0)
    span = jnp.where(kind == 0, 2, jnp.where(kind == 1, 4, jnp.where(kind == 2, 8, 16)))
    counts = jnp.minimum(place + 1, span).astype(F32)
    pooled = (window / counts - x[HALO:]).astype(BF16)
    out_ref[...] = (dot(pooled, mix_ref[...]) * scale_ref[...]).astype(BF16)


def step_map(later, carry, width):
    ch, cl = split(carry)
    linear = later[:, :width]
    moved = dot(linear, ch) + dot(linear, cl)
    offset = later[:, width:].astype(F32)
    return jnp.concatenate([moved[:, :width], moved[:, width:] + offset], axis=1)


def group_kernel(
    sp_ref, tp_ref, fs_ref, m0_ref, m1_ref, m2_ref, m3_ref, total_ref, linear_ref, offset_ref, before_ref, maps
):
    count, width, _ = maps.shape
    place = sp_ref[0] % count
    for d, piece in enumerate((m0_ref, m1_ref, m2_ref, m3_ref)):
        maps[(place + count - d) % count] = piece[...]
    r = lax.broadcasted_iota(jnp.int32, (width, width), 0)
    c = lax.broadcasted_iota(jnp.int32, (width, width), 1)
    eye = jnp.where(r == c, 1.0, 0.0)
    before = jnp.concatenate([eye, jnp.zeros((width, width), F32)], axis=1)
    carry = maps[0].astype(F32)
    for i in range(1, count):
        before = jnp.where(place == i, carry, before)
        carry = step_map(maps[i], carry, width)
    before_ref[...] = before
    total = carry.astype(BF16)
    total_ref[...] = total
    linear_ref[...] = total[:, :width]
    offset_ref[...] = total[:, width:]


def apply(linear, state):
    high, low = split(state)
    return dot(linear, high) + dot(linear, low)


def attend_kernel(
    sp_ref, tp_ref, fs_ref, t4_ref, a8_ref, b8_ref, b12_ref, before_ref, own_ref, eff_ref, silu_ref, gain_ref,
    pool_ref, wo_ref, mine_ref, other_ref,
):
    width = b8_ref.shape[0]
    state = apply(a8_ref[...], b12_ref[...].astype(F32)) + b8_ref[...].astype(F32)
    state = apply(t4_ref[:, :width], state) + t4_ref[:, width:].astype(F32)
    state = dot3(before_ref[:, :width], state) + before_ref[:, width:]
    attended = own_ref[...] + dot3(eff_ref[...], state)
    scale = lax.rsqrt(jnp.mean(attended * attended, axis=-1, keepdims=True) + EPS)
    delta = (attended * scale * gain_ref[...] * silu_ref[...]).astype(BF16)
    both = jnp.concatenate([pool_ref[...], delta], axis=1)
    core = tp_ref[0] % 2
    chips, rows, cols = mine_ref.shape
    step = 512
    for at in range(0, cols, step):
        part = dot(both, wo_ref[:, at : at + step]).astype(BF16)
        for j in range(chips):
            even = part[2 * j * rows : (2 * j + 1) * rows]
            odd = part[(2 * j + 1) * rows : (2 * j + 2) * rows]
            mine_ref[j, :, at : at + step] = jnp.where(core == 0, even, odd)
            other_ref[j, :, at : at + step] = jnp.where(core == 0, odd, even)


def pair_kernel(mine_ref, theirs_ref, out_ref):
    out_ref[...] = (mine_ref[...].astype(F32) + theirs_ref[...].astype(F32)).astype(BF16)


def sum_kernel(in_ref, out_ref):
    total = in_ref[0].astype(F32)
    for j in range(1, in_ref.shape[0]):
        total = total + in_ref[j].astype(F32)
    out_ref[...] = total.astype(BF16)


def layer(
    tokens,
    norm_gain,
    w_pool_in,
    w_query,
    w_key,
    w_value,
    w_gate,
    w_beta,
    w_decay,
    conv_weight,
    a_log,
    decay_extra,
    w_mix,
    pool_scale,
    delta_gain,
    w_out_pool,
    w_out_delta,
):
    n_sp = lax.axis_size("sp")
    n_tp = lax.axis_size("tp")
    sp_id = lax.axis_index("sp").astype(jnp.int32)
    tp_id = lax.axis_index("tp").astype(jnp.int32)
    fs_id = lax.axis_index("fs").astype(jnp.int32)
    ids = (sp_id[None], tp_id[None], fs_id[None])
    depth, width = w_key.shape
    rows, model = tokens.shape
    length = rows * n_tp
    half = depth // 2

    copies, part = call(
        start_kernel,
        (shape(n_tp, rows, model, dtype=BF16), shape(7 * depth // 4, width, dtype=BF16)),
        *ids, tokens, norm_gain,
        w_key, w_value, w_query, w_gate, w_pool_in, w_out_pool, w_out_delta,
        scratch=[pltpu.VMEM((3 * depth, width), BF16)], vmem=None,
    )
    all_rows = exchange(copies, "tp").reshape(length, model)
    tail = lax.ppermute(
        all_rows[length - HALO :], "sp", [(i, i + 1) for i in range(n_sp - 1)]
    )
    quarters = lax.all_gather(part, "sp", axis=0)
    kv = turns(quarters[:, :half], "fs", 4)
    rest = turns(quarters[:, half:], "fs", 4)

    xn, beta, gc, decay = call(
        gate_kernel,
        (
            shape(HALO + length, model, dtype=BF16),
            shape(length, 128),
            shape(length, 128),
            shape(length, length),
        ),
        *ids, a_log, all_rows, tail, w_beta.T, w_decay.T, decay_extra.T,
        smem=4, flops=2 * length * model * 128,
    )
    ab, keys, uw = call(
        local_kernel,
        (shape(width, 2 * width, dtype=BF16), shape(length, width), shape(length, 2 * width)),
        *ids, xn, *kv, conv_weight, beta, gc, decay,
        scratch=[
            pltpu.VMEM((model, 2 * width), BF16),
            pltpu.VMEM((HALO + length, width), F32),
            pltpu.VMEM((HALO + length, width), F32),
        ],
        flops=20 * length * model * width,
    )
    quad = 4
    near = turns(ab, "sp", quad)
    total, linear, offset, before = call(
        group_kernel,
        (
            shape(width, 2 * width, dtype=BF16),
            shape(width, width, dtype=BF16),
            shape(width, width, dtype=BF16),
            shape(width, 2 * width),
        ),
        *ids, *near,
        scratch=[pltpu.VMEM((quad, width, 2 * width), BF16)], flops=20 * width**3,
    )

    def from_behind(x, first, last, distance):
        return lax.ppermute(x, "sp", [(i, i + distance) for i in range(first, last)])

    t4 = from_behind(total, 0, n_sp - quad, quad)
    b8 = from_behind(offset, 0, n_sp - 2 * quad, 2 * quad)
    a8 = from_behind(linear, quad, n_sp - 2 * quad, 2 * quad)
    b12 = from_behind(offset, 0, n_sp - 3 * quad, 3 * quad)

    own, eff, silu_gate = call(
        query_kernel,
        (shape(length, width), shape(length, width), shape(length, width)),
        *ids, xn, *rest, conv_weight, gc, decay, keys, uw,
        scratch=[
            pltpu.VMEM((model, 2 * width), BF16),
            pltpu.VMEM((HALO + length, width), F32),
        ],
        flops=8 * length * model * width,
    )
    pool_out, w_mine = call(
        pool_kernel,
        (shape(length, width, dtype=BF16), shape(2 * width, model, dtype=BF16)),
        *ids, xn, *rest, w_mix[0], pool_scale.reshape(1, width),
        scratch=[
            pltpu.VMEM((3 * width, model), BF16),
            pltpu.VMEM((model, width), BF16),
            pltpu.VMEM((2 * HALO + length, width), F32),
            pltpu.VMEM((2 * HALO + length, width), F32),
        ],
        flops=8 * length * model * width,
    )
    chips = n_tp // 2
    mine, other = call(
        attend_kernel,
        (shape(chips, rows, model, dtype=BF16), shape(chips, rows, model, dtype=BF16)),
        *ids, t4, a8, b8, b12, before, own, eff, silu_gate, delta_gain.reshape(1, width), pool_out,
        w_mine,
        flops=4 * length * model * width,
    )
    theirs = lax.ppermute(other, "tp", [(i, i ^ 1) for i in range(n_tp)])
    partial = call(
        pair_kernel, shape(chips, rows, model, dtype=BF16), mine, theirs, smem=0, flops=1000000
    )
    cores = [[2 * x + c for x in range(chips)] for c in range(2)]
    arrived = exchange(partial, "tp", cores)
    return call(sum_kernel, shape(rows, model, dtype=BF16), arrived, smem=0, flops=1000000)


def solution(mesh):
    placed = (
        P(("fs", "sp", "tp"), None),
        P(),
        P("sp", "tp"),
        P("sp", "tp"),
        P("sp", "tp"),
        P("sp", "tp"),
        P("sp", "tp"),
        P(),
        P(),
        P(None, None, "tp"),
        P("tp"),
        P(("fs", "sp"), "tp"),
        P("tp", None, None),
        P("tp"),
        P(),
        P("tp", "sp"),
        P("tp", "sp"),
    )
    return jax.shard_map(
        layer,
        mesh=mesh,
        in_specs=placed,
        out_specs=P(("fs", "sp", "tp"), None),
        check_vma=False,
    )
```

```python
import jax
import jax.numpy as jnp
from jax import lax
from jax.experimental import pallas as pl
from jax.experimental.pallas import tpu as pltpu
from jax.sharding import PartitionSpec as P


EPS = 1e-06
HALO = 16
F32 = jnp.float32
BF16 = jnp.bfloat16


def call(kernel, outs, *args, smem=3, scratch=(), flops=0, vmem=16):
    in_specs = [pl.BlockSpec(memory_space=pltpu.SMEM)] * smem + [
        pl.BlockSpec(memory_space=pltpu.VMEM)
    ] * (len(args) - smem)
    many = isinstance(outs, (list, tuple))
    out_specs = pl.BlockSpec(memory_space=pltpu.VMEM)
    return pl.pallas_call(
        kernel,
        out_shape=list(outs) if many else outs,
        in_specs=in_specs,
        out_specs=[out_specs] * len(outs) if many else out_specs,
        scratch_shapes=list(scratch),
        compiler_params=pltpu.CompilerParams(vmem_limit_bytes=vmem and vmem * 1024 * 1024),
        cost_estimate=pl.CostEstimate(flops=flops, bytes_accessed=0, transcendentals=0),
    )(*args)


def shape(*dims, dtype=F32):
    return jax.ShapeDtypeStruct(dims, dtype)


def dot(a, b, dims=((1,), (0,))):
    return lax.dot_general(a, b, (dims, ((), ())), preferred_element_type=F32)


def split(a):
    high = a.astype(BF16)
    return high, (a - high.astype(F32)).astype(BF16)


def dot3(a, b, dims=((1,), (0,))):
    ah, al = split(a)
    bh, bl = split(b)
    return dot(ah, bh, dims) + (dot(ah, bl, dims) + dot(al, bh, dims))


def start_kernel(
    sp_ref, tp_ref, fs_ref, tok_ref, gain_ref, k_ref, v_ref, q_ref, g_ref, p_ref, op_ref, od_ref,
    copies_ref, part_ref, stacked,
):
    x = tok_ref[...].astype(F32)
    scale = lax.rsqrt(jnp.mean(x * x, axis=-1, keepdims=True) + EPS)
    gain = gain_ref[...].astype(F32).reshape(1, x.shape[1])
    normed = (x * scale * gain).astype(BF16)
    for j in range(copies_ref.shape[0]):
        copies_ref[j] = normed
    f = fs_ref[0]
    depth = k_ref.shape[0]
    half = depth // 2
    rows = pl.ds(pl.multiple_of((f % 2) * half, half), half)
    part_ref[0:half] = jnp.where(f < 2, k_ref[rows, :], v_ref[rows, :])
    part_ref[half:depth] = jnp.where(f < 2, q_ref[rows, :], g_ref[rows, :])
    stacked[0:depth] = p_ref[...]
    stacked[depth : 2 * depth] = op_ref[...]
    stacked[2 * depth :] = od_ref[...]
    third = 3 * depth // 4
    part_ref[depth:] = stacked[pl.ds(pl.multiple_of(f * third, 32), third), :]


def exchange(copies, axis, groups=None):
    return lax.all_to_all(
        copies, axis, split_axis=0, concat_axis=0, tiled=True, axis_index_groups=groups
    )


def turns(x, axis, size):
    n = lax.axis_size(axis)
    out = [x]
    for d in range(1, size):
        out.append(lax.ppermute(x, axis, [(i, i - i % size + (i + d) % size) for i in range(n)]))
    return out


def gate_kernel(
    sp_ref, tp_ref, fs_ref, a_log_ref, rows_ref, tail_ref, wb_ref, wd_ref, extra_ref,
    xn_ref, beta_ref, gc_ref, decay_ref,
):
    length = rows_ref.shape[0]
    tail = tail_ref[...]
    xn_ref[0:HALO] = jnp.where(sp_ref[0] > 0, tail, jnp.zeros_like(tail))
    xn_ref[HALO:] = rows_ref[...]
    lane = tp_ref[0]

    def own_column(w_ref):
        pre = dot(rows_ref[...], w_ref[...], ((1,), (1,)))
        col = lax.broadcasted_iota(jnp.int32, pre.shape, 1)
        return jnp.sum(jnp.where(col == lane, pre, 0.0), axis=1, keepdims=True)

    beta_pre, decay_pre = own_column(wb_ref), own_column(wd_ref)
    wide = (length, 128)
    beta_ref[...] = jax.nn.sigmoid(jnp.broadcast_to(beta_pre, wide))
    rate = jnp.exp(jnp.full(wide, a_log_ref[0], F32))
    soft = jax.nn.softplus(jnp.broadcast_to(decay_pre, wide))
    extra = jnp.transpose(jnp.broadcast_to(extra_ref[...], (128, length)))
    log_gate = -rate * soft + extra
    r = lax.broadcasted_iota(jnp.int32, (length, length), 0)
    c = lax.broadcasted_iota(jnp.int32, (length, length), 1)
    lower = jnp.where(r >= c, 1.0, 0.0).astype(BF16)
    g1 = log_gate.astype(BF16)
    rest = log_gate - g1.astype(F32)
    g2 = rest.astype(BF16)
    g3 = (rest - g2.astype(F32)).astype(BF16)
    gc = dot(lower, g1) + (dot(lower, g2) + dot(lower, g3))
    gc_ref[...] = gc
    across = jnp.transpose(gc)
    across = jnp.concatenate([across] * (length // 128), axis=0)
    along = jnp.concatenate([gc] * (length // 128), axis=1)
    gaps = along - across
    decay_ref[...] = jnp.where(r >= c, jnp.exp(jnp.where(r >= c, gaps, 0.0)), 0.0)


def gather_two(f, pieces, w_scr):
    count, _, width = pieces[0].shape
    half = width // 2
    for d, piece in enumerate(pieces):
        slot = (f + 4 - d) % 4
        cols = pl.ds(pl.multiple_of((slot // 2) * width, width), width)
        for s in range(count):
            at = pl.multiple_of((2 * s + slot % 2) * half, half)
            w_scr[pl.ds(at, half), cols] = piece[s, 0:half]


def short_conv(raw, taps, length, x_scr):
    x_scr[...] = raw.astype(BF16).astype(F32)
    conv = jnp.zeros((length, raw.shape[1]), F32)
    for j in range(4):
        conv = conv + x_scr[HALO - 3 + j : HALO - 3 + j + length, :] * taps[j : j + 1, :]
    return jax.nn.silu(conv)


def unit_rows(x):
    return x * lax.rsqrt(jnp.sum(x * x, axis=-1, keepdims=True) + EPS)


def inverse_unit_lower(low, size):
    r = lax.broadcasted_iota(jnp.int32, (size, size), 0)
    c = lax.broadcasted_iota(jnp.int32, (size, size), 1)
    inv = [jnp.where(r == c, 1.0, 0.0) - jnp.where((r // 2 == c // 2) & (r > c), x, 0.0) for x in low]
    b = 2
    while b < size:
        mask = (r // (2 * b) == c // (2 * b)) & (r % (2 * b) >= b) & (c % (2 * b) < b)
        mid = [dot3(x, jnp.where(mask, y, 0.0)) for x, y in zip(inv, low)]
        inv = [x - dot3(y, x) for x, y in zip(inv, mid)]
        b *= 2
    return inv


def local_kernel(
    sp_ref, tp_ref, fs_ref, xn_ref, w0_ref, w1_ref, w2_ref, w3_ref, taps_ref, beta_ref, gc_ref, decay_ref,
    ab_ref, k_ref, uw_ref,
    w_scr, k_scr, v_scr,
):
    length, width = k_ref.shape
    gather_two(fs_ref[0], (w0_ref, w1_ref, w2_ref, w3_ref), w_scr)
    raw = dot(xn_ref[...], w_scr[...])
    keys = unit_rows(short_conv(raw[:, :width], taps_ref[1], length, k_scr))
    values = short_conv(raw[:, width:], taps_ref[2], length, v_scr)
    k_ref[...] = keys
    beta = beta_ref[...]
    gc = gc_ref[...]
    kb = keys * beta
    r = lax.broadcasted_iota(jnp.int32, (length, length), 0)
    c = lax.broadcasted_iota(jnp.int32, (length, length), 1)
    corr = jnp.where(r > c, dot3(kb, keys, ((1,), (1,))) * decay_ref[...], 0.0)
    half = length // 2
    first, second = inverse_unit_lower(
        [corr[:half, :half], corr[half:, half:]], half
    )
    rhs = jnp.concatenate([values * beta, kb * jnp.exp(gc)], axis=1)
    top = dot3(first, rhs[:half])
    bottom = dot3(second, rhs[half:] - dot3(corr[half:, :half], top))
    uw_ref[0:half] = top
    uw_ref[half:] = bottom
    last = gc[length - 1 : length, :]
    kd = keys * jnp.exp(last - gc)
    made = dot3(kd, uw_ref[...], ((0,), (0,)))
    ri = lax.broadcasted_iota(jnp.int32, (width, width), 0)
    ci = lax.broadcasted_iota(jnp.int32, (width, width), 1)
    linear = jnp.where(ri == ci, jnp.exp(last), 0.0) - made[:, width:]
    ab_ref[:, :width] = linear.astype(BF16)
    ab_ref[:, width:] = made[:, :width].astype(BF16)


def query_kernel(
    sp_ref, tp_ref, fs_ref, xn_ref, w0_ref, w1_ref, w2_ref, w3_ref, taps_ref, gc_ref, decay_ref, k_ref, uw_ref,
    own_ref, eff_ref, silu_ref,
    w_scr, q_scr,
):
    length, width = k_ref.shape
    gather_two(fs_ref[0], (w0_ref, w1_ref, w2_ref, w3_ref), w_scr)
    raw = dot(xn_ref[...], w_scr[...])
    query = unit_rows(short_conv(raw[:, :width], taps_ref[0], length, q_scr)) * width ** (-0.5)
    silu_ref[...] = jax.nn.silu(raw[HALO:, width:].astype(BF16).astype(F32))
    scores = dot3(query, k_ref[...], ((1,), (1,))) * decay_ref[...]
    both = dot3(scores, uw_ref[...])
    own_ref[...] = both[:, :width]
    eff_ref[...] = query * jnp.exp(gc_ref[...]) - both[:, width:]


def pool_kernel(
    sp_ref, tp_ref, fs_ref, xn_ref, w0_ref, w1_ref, w2_ref, w3_ref, mix_ref, scale_ref,
    out_ref, wo_ref, w_all, w_scr, a_scr, b_scr,
):
    count, part, width = w0_ref.shape
    skip = width // 2
    part = part - skip
    length = xn_ref.shape[0] - HALO
    for d, piece in enumerate((w0_ref, w1_ref, w2_ref, w3_ref)):
        at = pl.multiple_of(((fs_ref[0] + 4 - d) % 4) * part, 32)
        for s in range(count):
            w_all[pl.ds(at, part), s * width : (s + 1) * width] = piece[s, skip:]
    for s in range(count):
        w_scr[s * width : (s + 1) * width, :] = w_all[0:width, s * width : (s + 1) * width]
    wo_ref[...] = w_all[width:, :]
    x = dot(xn_ref[...], w_scr[...]).astype(BF16).astype(F32)
    kind = tp_ref[0] % 4
    total = HALO + length
    a_scr[0:HALO] = jnp.zeros((HALO, width), F32)
    b_scr[0:HALO] = jnp.zeros((HALO, width), F32)
    a_scr[HALO:] = x
    two = x + a_scr[HALO - 1 : HALO - 1 + total]
    b_scr[HALO:] = two
    four = two + b_scr[HALO - 2 : HALO - 2 + total]
    a_scr[HALO:] = four
    eight = four + a_scr[HALO - 4 : HALO - 4 + total]
    b_scr[HALO:] = eight
    sixteen = eight + b_scr[HALO - 8 : HALO - 8 + total]
    window = jnp.where(kind == 0, two, jnp.where(kind == 1, four, jnp.where(kind == 2, eight, sixteen)))
    window = window[HALO:]
    place = sp_ref[0] * length + lax.broadcasted_iota(jnp.int32, (length, width), 0)
    span = jnp.where(kind == 0, 2, jnp.where(kind == 1, 4, jnp.where(kind == 2, 8, 16)))
    counts = jnp.minimum(place + 1, span).astype(F32)
    pooled = (window / counts - x[HALO:]).astype(BF16)
    out_ref[...] = (dot(pooled, mix_ref[...]) * scale_ref[...]).astype(BF16)


def step_map(later, carry, width):
    ch, cl = split(carry)
    linear = later[:, :width]
    moved = dot(linear, ch) + dot(linear, cl)
    offset = later[:, width:].astype(F32)
    return jnp.concatenate([moved[:, :width], moved[:, width:] + offset], axis=1)


def pair_map_kernel(sp_ref, tp_ref, fs_ref, own_ref, other_ref, pair_ref, before_ref):
    width = own_ref.shape[0]
    odd = sp_ref[0] % 2 == 1
    own, other = own_ref[...], other_ref[...]
    earlier = jnp.where(odd, other, own)
    later = jnp.where(odd, own, other)
    pair_ref[...] = step_map(later, earlier.astype(F32), width).astype(BF16)
    r = lax.broadcasted_iota(jnp.int32, (width, 2 * width), 0)
    c = lax.broadcasted_iota(jnp.int32, (width, 2 * width), 1)
    before_ref[...] = jnp.where(odd, other, jnp.where(r == c, 1.0, 0.0).astype(BF16))


def group_kernel(
    sp_ref, tp_ref, fs_ref, own_ref, other_ref, inner_ref,
    total_ref, linear_ref, offset_ref, before_ref,
):
    width = own_ref.shape[0]
    upper = (sp_ref[0] // 2) % 2 == 1
    own, other = own_ref[...], other_ref[...]
    earlier = jnp.where(upper, other, own)
    later = jnp.where(upper, own, other)
    total = step_map(later, earlier.astype(F32), width).astype(BF16)
    total_ref[...] = total
    linear_ref[...] = total[:, :width]
    offset_ref[...] = total[:, width:]
    inner = inner_ref[...]
    behind = step_map(inner, other.astype(F32), width)
    before_ref[...] = jnp.where(upper, behind, inner.astype(F32))


def apply(linear, state):
    high, low = split(state)
    return dot(linear, high) + dot(linear, low)


def attend_kernel(
    sp_ref, tp_ref, fs_ref, t4_ref, a8_ref, b8_ref, b12_ref, before_ref, own_ref, eff_ref, silu_ref, gain_ref,
    pool_ref, wo_ref, mine_ref, other_ref,
):
    width = b8_ref.shape[0]
    state = apply(a8_ref[...], b12_ref[...].astype(F32)) + b8_ref[...].astype(F32)
    state = apply(t4_ref[:, :width], state) + t4_ref[:, width:].astype(F32)
    state = dot3(before_ref[:, :width], state) + before_ref[:, width:]
    attended = own_ref[...] + dot3(eff_ref[...], state)
    scale = lax.rsqrt(jnp.mean(attended * attended, axis=-1, keepdims=True) + EPS)
    delta = (attended * scale * gain_ref[...] * silu_ref[...]).astype(BF16)
    both = jnp.concatenate([pool_ref[...], delta], axis=1)
    core = tp_ref[0] % 2
    chips, rows, cols = mine_ref.shape
    step = 512
    for at in range(0, cols, step):
        part = dot(both, wo_ref[:, at : at + step]).astype(BF16)
        for j in range(chips):
            even = part[2 * j * rows : (2 * j + 1) * rows]
            odd = part[(2 * j + 1) * rows : (2 * j + 2) * rows]
            mine_ref[j, :, at : at + step] = jnp.where(core == 0, even, odd)
            other_ref[j, :, at : at + step] = jnp.where(core == 0, odd, even)


def pair_kernel(mine_ref, theirs_ref, out_ref):
    out_ref[...] = (mine_ref[...].astype(F32) + theirs_ref[...].astype(F32)).astype(BF16)


def sum_kernel(in_ref, out_ref):
    total = in_ref[0].astype(F32)
    for j in range(1, in_ref.shape[0]):
        total = total + in_ref[j].astype(F32)
    out_ref[...] = total.astype(BF16)


def layer(
    tokens,
    norm_gain,
    w_pool_in,
    w_query,
    w_key,
    w_value,
    w_gate,
    w_beta,
    w_decay,
    conv_weight,
    a_log,
    decay_extra,
    w_mix,
    pool_scale,
    delta_gain,
    w_out_pool,
    w_out_delta,
):
    n_sp = lax.axis_size("sp")
    n_tp = lax.axis_size("tp")
    sp_id = lax.axis_index("sp").astype(jnp.int32)
    tp_id = lax.axis_index("tp").astype(jnp.int32)
    fs_id = lax.axis_index("fs").astype(jnp.int32)
    ids = (sp_id[None], tp_id[None], fs_id[None])
    depth, width = w_key.shape
    rows, model = tokens.shape
    length = rows * n_tp
    half = depth // 2

    copies, part = call(
        start_kernel,
        (shape(n_tp, rows, model, dtype=BF16), shape(7 * depth // 4, width, dtype=BF16)),
        *ids, tokens, norm_gain,
        w_key, w_value, w_query, w_gate, w_pool_in, w_out_pool, w_out_delta,
        scratch=[pltpu.VMEM((3 * depth, width), BF16)], vmem=None,
    )
    all_rows = exchange(copies, "tp").reshape(length, model)
    tail = lax.ppermute(
        all_rows[length - HALO :], "sp", [(i, i + 1) for i in range(n_sp - 1)]
    )
    quarters = lax.all_gather(part, "sp", axis=0)
    kv = turns(quarters[:, :half], "fs", 4)
    rest = turns(quarters[:, half:], "fs", 4)

    xn, beta, gc, decay = call(
        gate_kernel,
        (
            shape(HALO + length, model, dtype=BF16),
            shape(length, 128),
            shape(length, 128),
            shape(length, length),
        ),
        *ids, a_log, all_rows, tail, w_beta.T, w_decay.T, decay_extra.T,
        smem=4, flops=2 * length * model * 128,
    )
    ab, keys, uw = call(
        local_kernel,
        (shape(width, 2 * width, dtype=BF16), shape(length, width), shape(length, 2 * width)),
        *ids, xn, *kv, conv_weight, beta, gc, decay,
        scratch=[
            pltpu.VMEM((model, 2 * width), BF16),
            pltpu.VMEM((HALO + length, width), F32),
            pltpu.VMEM((HALO + length, width), F32),
        ],
        flops=20 * length * model * width,
    )
    quad = 4

    def meet(x, distance):
        return lax.ppermute(x, "sp", [(i, i ^ distance) for i in range(n_sp)])

    pair, inner = call(
        pair_map_kernel,
        (shape(width, 2 * width, dtype=BF16), shape(width, 2 * width, dtype=BF16)),
        *ids, ab, meet(ab, 1),
        flops=20 * width**3,
    )
    total, linear, offset, before = call(
        group_kernel,
        (
            shape(width, 2 * width, dtype=BF16),
            shape(width, width, dtype=BF16),
            shape(width, width, dtype=BF16),
            shape(width, 2 * width),
        ),
        *ids, pair, meet(pair, 2), inner,
        flops=20 * width**3,
    )

    def from_behind(x, first, last, distance):
        return lax.ppermute(x, "sp", [(i, i + distance) for i in range(first, last)])

    t4 = from_behind(total, 0, n_sp - quad, quad)
    b8 = from_behind(offset, 0, n_sp - 2 * quad, 2 * quad)
    a8 = from_behind(linear, quad, n_sp - 2 * quad, 2 * quad)
    b12 = from_behind(offset, 0, n_sp - 3 * quad, 3 * quad)

    own, eff, silu_gate = call(
        query_kernel,
        (shape(length, width), shape(length, width), shape(length, width)),
        *ids, xn, *rest, conv_weight, gc, decay, keys, uw,
        scratch=[
            pltpu.VMEM((model, 2 * width), BF16),
            pltpu.VMEM((HALO + length, width), F32),
        ],
        flops=8 * length * model * width,
    )
    pool_out, w_mine = call(
        pool_kernel,
        (shape(length, width, dtype=BF16), shape(2 * width, model, dtype=BF16)),
        *ids, xn, *rest, w_mix[0], pool_scale.reshape(1, width),
        scratch=[
            pltpu.VMEM((3 * width, model), BF16),
            pltpu.VMEM((model, width), BF16),
            pltpu.VMEM((2 * HALO + length, width), F32),
            pltpu.VMEM((2 * HALO + length, width), F32),
        ],
        flops=8 * length * model * width,
    )
    chips = n_tp // 2
    mine, other = call(
        attend_kernel,
        (shape(chips, rows, model, dtype=BF16), shape(chips, rows, model, dtype=BF16)),
        *ids, t4, a8, b8, b12, before, own, eff, silu_gate, delta_gain.reshape(1, width), pool_out,
        w_mine,
        flops=4 * length * model * width,
    )
    theirs = lax.ppermute(other, "tp", [(i, i ^ 1) for i in range(n_tp)])
    partial = call(
        pair_kernel, shape(chips, rows, model, dtype=BF16), mine, theirs, smem=0, flops=1000000
    )
    cores = [[2 * x + c for x in range(chips)] for c in range(2)]
    arrived = exchange(partial, "tp", cores)
    return call(sum_kernel, shape(rows, model, dtype=BF16), arrived, smem=0, flops=1000000)


def solution(mesh):
    placed = (
        P(("fs", "sp", "tp"), None),
        P(),
        P("sp", "tp"),
        P("sp", "tp"),
        P("sp", "tp"),
        P("sp", "tp"),
        P("sp", "tp"),
        P(),
        P(),
        P(None, None, "tp"),
        P("tp"),
        P(("fs", "sp"), "tp"),
        P("tp", None, None),
        P("tp"),
        P(),
        P("tp", "sp"),
        P("tp", "sp"),
    )
    return jax.shard_map(
        layer,
        mesh=mesh,
        in_specs=placed,
        out_specs=P(("fs", "sp", "tp"), None),
        check_vma=False,
    )
```

```python
import jax
import jax.numpy as jnp
from jax import lax
from jax.experimental import pallas as pl
from jax.experimental.pallas import tpu as pltpu
from jax.sharding import PartitionSpec as P


EPS = 1e-06
HALO = 16
F32 = jnp.float32
BF16 = jnp.bfloat16


def call(kernel, outs, *args, smem=3, scratch=(), flops=0, vmem=16):
    in_specs = [pl.BlockSpec(memory_space=pltpu.SMEM)] * smem + [
        pl.BlockSpec(memory_space=pltpu.VMEM)
    ] * (len(args) - smem)
    many = isinstance(outs, (list, tuple))
    out_specs = pl.BlockSpec(memory_space=pltpu.VMEM)
    return pl.pallas_call(
        kernel,
        out_shape=list(outs) if many else outs,
        in_specs=in_specs,
        out_specs=[out_specs] * len(outs) if many else out_specs,
        scratch_shapes=list(scratch),
        compiler_params=pltpu.CompilerParams(vmem_limit_bytes=vmem and vmem * 1024 * 1024),
        cost_estimate=pl.CostEstimate(flops=flops, bytes_accessed=0, transcendentals=0),
    )(*args)


def shape(*dims, dtype=F32):
    return jax.ShapeDtypeStruct(dims, dtype)


def dot(a, b, dims=((1,), (0,))):
    return lax.dot_general(a, b, (dims, ((), ())), preferred_element_type=F32)


def split(a):
    high = a.astype(BF16)
    return high, (a - high.astype(F32)).astype(BF16)


def dot3(a, b, dims=((1,), (0,))):
    ah, al = split(a)
    bh, bl = split(b)
    return dot(ah, bh, dims) + (dot(ah, bl, dims) + dot(al, bh, dims))


def product(a, b):
    (ah, al), (bh, bl) = a, b
    return dot(jnp.concatenate([ah, al], axis=1), jnp.concatenate([bh, bh], axis=0)) + dot(ah, bl)


def start_kernel(
    sp_ref, tp_ref, fs_ref, tok_ref, gain_ref, k_ref, v_ref, q_ref, g_ref, p_ref, op_ref, od_ref,
    copies_ref, part_ref, stacked,
):
    x = tok_ref[...].astype(F32)
    scale = lax.rsqrt(jnp.mean(x * x, axis=-1, keepdims=True) + EPS)
    gain = gain_ref[...].astype(F32).reshape(1, x.shape[1])
    normed = (x * scale * gain).astype(BF16)
    for j in range(copies_ref.shape[0]):
        copies_ref[j] = normed
    f = fs_ref[0]
    depth = k_ref.shape[0]
    half = depth // 2
    rows = pl.ds(pl.multiple_of((f % 2) * half, half), half)
    part_ref[0:half] = jnp.where(f < 2, k_ref[rows, :], v_ref[rows, :])
    part_ref[half:depth] = jnp.where(f < 2, q_ref[rows, :], g_ref[rows, :])
    stacked[0:depth] = p_ref[...]
    stacked[depth : 2 * depth] = op_ref[...]
    stacked[2 * depth :] = od_ref[...]
    third = 3 * depth // 4
    part_ref[depth:] = stacked[pl.ds(pl.multiple_of(f * third, 32), third), :]


def exchange(copies, axis, groups=None):
    return lax.all_to_all(
        copies, axis, split_axis=0, concat_axis=0, tiled=True, axis_index_groups=groups
    )


def turns(x, axis, size):
    n = lax.axis_size(axis)
    out = [x]
    for d in range(1, size):
        out.append(lax.ppermute(x, axis, [(i, i - i % size + (i + d) % size) for i in range(n)]))
    return out


def gate_kernel(
    sp_ref, tp_ref, fs_ref, a_log_ref, rows_ref, tail_ref, wb_ref, wd_ref, extra_ref,
    xn_ref, beta_ref, gc_ref, decay_ref,
):
    length = rows_ref.shape[0]
    tail = tail_ref[...]
    xn_ref[0:HALO] = jnp.where(sp_ref[0] > 0, tail, jnp.zeros_like(tail))
    xn_ref[HALO:] = rows_ref[...]
    lane = tp_ref[0]

    def own_column(w_ref):
        pre = dot(rows_ref[...], w_ref[...], ((1,), (1,)))
        col = lax.broadcasted_iota(jnp.int32, pre.shape, 1)
        return jnp.sum(jnp.where(col == lane, pre, 0.0), axis=1, keepdims=True)

    beta_pre, decay_pre = own_column(wb_ref), own_column(wd_ref)
    wide = (length, 128)
    beta_ref[...] = jax.nn.sigmoid(jnp.broadcast_to(beta_pre, wide))
    rate = jnp.exp(jnp.full(wide, a_log_ref[0], F32))
    soft = jax.nn.softplus(jnp.broadcast_to(decay_pre, wide))
    extra = jnp.transpose(jnp.broadcast_to(extra_ref[...], (128, length)))
    log_gate = -rate * soft + extra
    r = lax.broadcasted_iota(jnp.int32, (length, length), 0)
    c = lax.broadcasted_iota(jnp.int32, (length, length), 1)
    lower = jnp.where(r >= c, 1.0, 0.0).astype(BF16)
    g1 = log_gate.astype(BF16)
    rest = log_gate - g1.astype(F32)
    g2 = rest.astype(BF16)
    g3 = (rest - g2.astype(F32)).astype(BF16)
    gc = dot(lower, g1) + (dot(lower, g2) + dot(lower, g3))
    gc_ref[...] = gc
    across = jnp.transpose(gc)
    across = jnp.concatenate([across] * (length // 128), axis=0)
    along = jnp.concatenate([gc] * (length // 128), axis=1)
    gaps = along - across
    decay_ref[...] = jnp.where(r >= c, jnp.exp(jnp.where(r >= c, gaps, 0.0)), 0.0)


def gather_two(f, pieces, w_scr):
    count, _, width = pieces[0].shape
    half = width // 2
    for d, piece in enumerate(pieces):
        slot = (f + 4 - d) % 4
        cols = pl.ds(pl.multiple_of((slot // 2) * width, width), width)
        for s in range(count):
            at = pl.multiple_of((2 * s + slot % 2) * half, half)
            w_scr[pl.ds(at, half), cols] = piece[s, 0:half]


def short_conv(raw, taps, length, x_scr):
    x_scr[...] = raw.astype(BF16).astype(F32)
    conv = jnp.zeros((length, raw.shape[1]), F32)
    for j in range(4):
        conv = conv + x_scr[HALO - 3 + j : HALO - 3 + j + length, :] * taps[j : j + 1, :]
    return jax.nn.silu(conv)


def unit_rows(x):
    return x * lax.rsqrt(jnp.sum(x * x, axis=-1, keepdims=True) + EPS)


def inverse_unit_lower(low, size):
    r = lax.broadcasted_iota(jnp.int32, (size, size), 0)
    c = lax.broadcasted_iota(jnp.int32, (size, size), 1)
    apart = r ^ c
    inv = [jnp.where(apart == 0, 1.0, jnp.where(apart == 1, -x, 0.0)) for x in low]
    b = 2
    while b < size:
        here = (apart >= b) & (apart < 2 * b)
        parts = [split(x) for x in inv]
        mid = [product(x, split(jnp.where(here, y, 0.0))) for x, y in zip(parts, low)]
        inv = [x - product(split(y), p) for x, y, p in zip(inv, mid, parts)]
        b *= 2
    return inv


def local_kernel(
    sp_ref, tp_ref, fs_ref, xn_ref, w0_ref, w1_ref, w2_ref, w3_ref, taps_ref, beta_ref, gc_ref, decay_ref,
    ab_ref, k_ref, uw_ref,
    w_scr, k_scr, v_scr,
):
    length, width = k_ref.shape
    gather_two(fs_ref[0], (w0_ref, w1_ref, w2_ref, w3_ref), w_scr)
    raw = dot(xn_ref[...], w_scr[...])
    keys = unit_rows(short_conv(raw[:, :width], taps_ref[1], length, k_scr))
    values = short_conv(raw[:, width:], taps_ref[2], length, v_scr)
    k_ref[...] = keys
    beta = beta_ref[...]
    gc = gc_ref[...]
    kb = keys * beta
    r = lax.broadcasted_iota(jnp.int32, (length, length), 0)
    c = lax.broadcasted_iota(jnp.int32, (length, length), 1)
    corr = jnp.where(r > c, dot3(kb, keys, ((1,), (1,))) * decay_ref[...], 0.0)
    half = length // 2
    first, second = inverse_unit_lower(
        [corr[:half, :half], corr[half:, half:]], half
    )
    rhs = jnp.concatenate([values * beta, kb * jnp.exp(gc)], axis=1)
    top = dot3(first, rhs[:half])
    bottom = dot3(second, rhs[half:] - dot3(corr[half:, :half], top))
    uw_ref[0:half] = top
    uw_ref[half:] = bottom
    last = gc[length - 1 : length, :]
    kd = keys * jnp.exp(last - gc)
    made = dot3(kd, uw_ref[...], ((0,), (0,)))
    ri = lax.broadcasted_iota(jnp.int32, (width, width), 0)
    ci = lax.broadcasted_iota(jnp.int32, (width, width), 1)
    linear = jnp.where(ri == ci, jnp.exp(last), 0.0) - made[:, width:]
    ab_ref[:, :width] = linear.astype(BF16)
    ab_ref[:, width:] = made[:, :width].astype(BF16)


def step_map(later, carry, width):
    ch, cl = split(carry)
    linear = later[:, :width]
    moved = dot(linear, ch) + dot(linear, cl)
    offset = later[:, width:].astype(F32)
    return jnp.concatenate([moved[:, :width], moved[:, width:] + offset], axis=1)


def pair_map_kernel(sp_ref, tp_ref, fs_ref, own_ref, other_ref, pair_ref, before_ref):
    width = own_ref.shape[0]
    odd = sp_ref[0] % 2 == 1
    own, other = own_ref[...], other_ref[...]
    earlier = jnp.where(odd, other, own)
    later = jnp.where(odd, own, other)
    pair_ref[...] = step_map(later, earlier.astype(F32), width).astype(BF16)
    r = lax.broadcasted_iota(jnp.int32, (width, 2 * width), 0)
    c = lax.broadcasted_iota(jnp.int32, (width, 2 * width), 1)
    before_ref[...] = jnp.where(odd, other, jnp.where(r == c, 1.0, 0.0).astype(BF16))


def group_kernel(
    sp_ref, tp_ref, fs_ref, own_ref, other_ref, inner_ref,
    total_ref, linear_ref, offset_ref, before_ref,
):
    width = own_ref.shape[0]
    upper = (sp_ref[0] // 2) % 2 == 1
    own, other = own_ref[...], other_ref[...]
    earlier = jnp.where(upper, other, own)
    later = jnp.where(upper, own, other)
    total = step_map(later, earlier.astype(F32), width).astype(BF16)
    total_ref[...] = total
    linear_ref[...] = total[:, :width]
    offset_ref[...] = total[:, width:]
    inner = inner_ref[...]
    behind = step_map(inner, other.astype(F32), width)
    before_ref[...] = jnp.where(upper, behind, inner.astype(F32))


def apply(linear, state):
    high, low = split(state)
    return dot(linear, high) + dot(linear, low)


def output_kernel(
    sp_ref, tp_ref, fs_ref, xn_ref, w0_ref, w1_ref, w2_ref, w3_ref, taps_ref, gc_ref, decay_ref,
    k_ref, uw_ref, mix_ref, scale_ref, t4_ref, a8_ref, b8_ref, b12_ref, before_ref, gain_ref,
    mine_ref, other_ref,
    w_scr, w_all, q_scr, a_scr, b_scr,
):
    length, width = k_ref.shape
    pieces = (w0_ref, w1_ref, w2_ref, w3_ref)
    state = apply(a8_ref[...], b12_ref[...].astype(F32)) + b8_ref[...].astype(F32)
    state = apply(t4_ref[:, :width], state) + t4_ref[:, width:].astype(F32)
    state = dot3(before_ref[:, :width], state) + before_ref[:, width:]
    gather_two(fs_ref[0], pieces, w_scr)
    count, part, _ = w0_ref.shape
    skip = width // 2
    part = part - skip
    for d, piece in enumerate(pieces):
        at = pl.multiple_of(((fs_ref[0] + 4 - d) % 4) * part, 32)
        for s in range(count):
            w_all[pl.ds(at, part), s * width : (s + 1) * width] = piece[s, skip:]
    for s in range(count):
        w_scr[s * width : (s + 1) * width, 2 * width :] = w_all[
            0:width, s * width : (s + 1) * width
        ]
    raw = dot(xn_ref[...], w_scr[...])
    query = unit_rows(short_conv(raw[:, :width], taps_ref[0], length, q_scr)) * width ** (-0.5)
    silu_gate = jax.nn.silu(raw[HALO:, width : 2 * width].astype(BF16).astype(F32))
    scores = dot3(query, k_ref[...], ((1,), (1,))) * decay_ref[...]
    both = dot3(scores, uw_ref[...])
    effect = query * jnp.exp(gc_ref[...]) - both[:, width:]
    attended = both[:, :width] + dot3(effect, state)
    scale = lax.rsqrt(jnp.mean(attended * attended, axis=-1, keepdims=True) + EPS)
    delta = (attended * scale * gain_ref[...] * silu_gate).astype(BF16)
    x = raw[:, 2 * width :].astype(BF16).astype(F32)
    kind = tp_ref[0] % 4
    total = HALO + length
    a_scr[0:HALO] = jnp.zeros((HALO, width), F32)
    b_scr[0:HALO] = jnp.zeros((HALO, width), F32)
    a_scr[HALO:] = x
    two = x + a_scr[HALO - 1 : HALO - 1 + total]
    b_scr[HALO:] = two
    four = two + b_scr[HALO - 2 : HALO - 2 + total]
    a_scr[HALO:] = four
    eight = four + a_scr[HALO - 4 : HALO - 4 + total]
    b_scr[HALO:] = eight
    sixteen = eight + b_scr[HALO - 8 : HALO - 8 + total]
    window = jnp.where(
        kind == 0, two, jnp.where(kind == 1, four, jnp.where(kind == 2, eight, sixteen))
    )
    window = window[HALO:]
    place = sp_ref[0] * length + lax.broadcasted_iota(jnp.int32, (length, width), 0)
    span = jnp.where(kind == 0, 2, jnp.where(kind == 1, 4, jnp.where(kind == 2, 8, 16)))
    counts = jnp.minimum(place + 1, span).astype(F32)
    pooled = (window / counts - x[HALO:]).astype(BF16)
    pool_out = (dot(pooled, mix_ref[...]) * scale_ref[...]).astype(BF16)
    channels = jnp.concatenate([pool_out, delta], axis=1)
    core = tp_ref[0] % 2
    chips, rows, cols = mine_ref.shape
    step = 512
    for at in range(0, cols, step):
        made = dot(channels, w_all[width:, at : at + step]).astype(BF16)
        for j in range(chips):
            even = made[2 * j * rows : (2 * j + 1) * rows]
            odd = made[(2 * j + 1) * rows : (2 * j + 2) * rows]
            mine_ref[j, :, at : at + step] = jnp.where(core == 0, even, odd)
            other_ref[j, :, at : at + step] = jnp.where(core == 0, odd, even)


def pair_kernel(mine_ref, theirs_ref, out_ref):
    out_ref[...] = (mine_ref[...].astype(F32) + theirs_ref[...].astype(F32)).astype(BF16)


def sum_kernel(in_ref, out_ref):
    total = in_ref[0].astype(F32)
    for j in range(1, in_ref.shape[0]):
        total = total + in_ref[j].astype(F32)
    out_ref[...] = total.astype(BF16)


def layer(
    tokens,
    norm_gain,
    w_pool_in,
    w_query,
    w_key,
    w_value,
    w_gate,
    w_beta,
    w_decay,
    conv_weight,
    a_log,
    decay_extra,
    w_mix,
    pool_scale,
    delta_gain,
    w_out_pool,
    w_out_delta,
):
    n_sp = lax.axis_size("sp")
    n_tp = lax.axis_size("tp")
    sp_id = lax.axis_index("sp").astype(jnp.int32)
    tp_id = lax.axis_index("tp").astype(jnp.int32)
    fs_id = lax.axis_index("fs").astype(jnp.int32)
    ids = (sp_id[None], tp_id[None], fs_id[None])
    depth, width = w_key.shape
    rows, model = tokens.shape
    length = rows * n_tp
    half = depth // 2

    copies, part = call(
        start_kernel,
        (shape(n_tp, rows, model, dtype=BF16), shape(7 * depth // 4, width, dtype=BF16)),
        *ids, tokens, norm_gain,
        w_key, w_value, w_query, w_gate, w_pool_in, w_out_pool, w_out_delta,
        scratch=[pltpu.VMEM((3 * depth, width), BF16)], vmem=None,
    )
    all_rows = exchange(copies, "tp").reshape(length, model)
    tail = lax.ppermute(
        all_rows[length - HALO :], "sp", [(i, i + 1) for i in range(n_sp - 1)]
    )
    quarters = lax.all_gather(part, "sp", axis=0)
    kv = turns(quarters[:, :half], "fs", 4)
    rest = turns(quarters[:, half:], "fs", 4)

    xn, beta, gc, decay = call(
        gate_kernel,
        (
            shape(HALO + length, model, dtype=BF16),
            shape(length, 128),
            shape(length, 128),
            shape(length, length),
        ),
        *ids, a_log, all_rows, tail, w_beta.T, w_decay.T, decay_extra.T,
        smem=4, flops=2 * length * model * 128,
    )
    ab, keys, uw = call(
        local_kernel,
        (shape(width, 2 * width, dtype=BF16), shape(length, width), shape(length, 2 * width)),
        *ids, xn, *kv, conv_weight, beta, gc, decay,
        scratch=[
            pltpu.VMEM((model, 2 * width), BF16),
            pltpu.VMEM((HALO + length, width), F32),
            pltpu.VMEM((HALO + length, width), F32),
        ],
        flops=20 * length * model * width,
    )
    quad = 4

    def meet(x, distance):
        return lax.ppermute(x, "sp", [(i, i ^ distance) for i in range(n_sp)])

    pair, inner = call(
        pair_map_kernel,
        (shape(width, 2 * width, dtype=BF16), shape(width, 2 * width, dtype=BF16)),
        *ids, ab, meet(ab, 1),
        flops=20 * width**3,
    )
    total, linear, offset, before = call(
        group_kernel,
        (
            shape(width, 2 * width, dtype=BF16),
            shape(width, width, dtype=BF16),
            shape(width, width, dtype=BF16),
            shape(width, 2 * width),
        ),
        *ids, pair, meet(pair, 2), inner,
        flops=20 * width**3,
    )

    def from_behind(x, first, last, distance):
        return lax.ppermute(x, "sp", [(i, i + distance) for i in range(first, last)])

    t4 = from_behind(total, 0, n_sp - quad, quad)
    b8 = from_behind(offset, 0, n_sp - 2 * quad, 2 * quad)
    a8 = from_behind(linear, quad, n_sp - 2 * quad, 2 * quad)
    b12 = from_behind(offset, 0, n_sp - 3 * quad, 3 * quad)

    chips = n_tp // 2
    mine, other = call(
        output_kernel,
        (shape(chips, rows, model, dtype=BF16), shape(chips, rows, model, dtype=BF16)),
        *ids, xn, *rest, conv_weight, gc, decay, keys, uw, w_mix[0], pool_scale.reshape(1, width),
        t4, a8, b8, b12, before, delta_gain.reshape(1, width),
        scratch=[
            pltpu.VMEM((model, 3 * width), BF16),
            pltpu.VMEM((3 * width, model), BF16),
            pltpu.VMEM((HALO + length, width), F32),
            pltpu.VMEM((2 * HALO + length, width), F32),
            pltpu.VMEM((2 * HALO + length, width), F32),
        ],
        flops=20 * length * model * width,
    )
    theirs = lax.ppermute(other, "tp", [(i, i ^ 1) for i in range(n_tp)])
    partial = call(
        pair_kernel, shape(chips, rows, model, dtype=BF16), mine, theirs, smem=0, flops=1000000
    )
    cores = [[2 * x + c for x in range(chips)] for c in range(2)]
    arrived = exchange(partial, "tp", cores)
    return call(sum_kernel, shape(rows, model, dtype=BF16), arrived, smem=0, flops=1000000)


def solution(mesh):
    placed = (
        P(("fs", "sp", "tp"), None),
        P(),
        P("sp", "tp"),
        P("sp", "tp"),
        P("sp", "tp"),
        P("sp", "tp"),
        P("sp", "tp"),
        P(),
        P(),
        P(None, None, "tp"),
        P("tp"),
        P(("fs", "sp"), "tp"),
        P("tp", None, None),
        P("tp"),
        P(),
        P("tp", "sp"),
        P("tp", "sp"),
    )
    return jax.shard_map(
        layer,
        mesh=mesh,
        in_specs=placed,
        out_specs=P(("fs", "sp", "tp"), None),
        check_vma=False,
    )
```

```python
import jax
import jax.numpy as jnp
from jax import lax
from jax.experimental import pallas as pl
from jax.experimental.pallas import tpu as pltpu
from jax.sharding import PartitionSpec as P


EPS = 1e-06
HALO = 16
F32 = jnp.float32
BF16 = jnp.bfloat16


def call(kernel, outs, *args, smem=3, scratch=(), flops=0, vmem=16):
    in_specs = [pl.BlockSpec(memory_space=pltpu.SMEM)] * smem + [
        pl.BlockSpec(memory_space=pltpu.VMEM)
    ] * (len(args) - smem)
    many = isinstance(outs, (list, tuple))
    out_specs = pl.BlockSpec(memory_space=pltpu.VMEM)
    return pl.pallas_call(
        kernel,
        out_shape=list(outs) if many else outs,
        in_specs=in_specs,
        out_specs=[out_specs] * len(outs) if many else out_specs,
        scratch_shapes=list(scratch),
        compiler_params=pltpu.CompilerParams(vmem_limit_bytes=vmem and vmem * 1024 * 1024),
        cost_estimate=pl.CostEstimate(flops=flops, bytes_accessed=0, transcendentals=0),
    )(*args)


def shape(*dims, dtype=F32):
    return jax.ShapeDtypeStruct(dims, dtype)


def dot(a, b, dims=((1,), (0,))):
    return lax.dot_general(a, b, (dims, ((), ())), preferred_element_type=F32)


def split(a):
    high = a.astype(BF16)
    return high, (a - high.astype(F32)).astype(BF16)


def dot1(a, b, dims=((1,), (0,))):
    return dot(a.astype(BF16), b.astype(BF16), dims)


def dot3(a, b, dims=((1,), (0,))):
    ah, al = split(a)
    bh, bl = split(b)
    return dot(ah, bh, dims) + (dot(ah, bl, dims) + dot(al, bh, dims))


def product(a, b):
    (ah, al), (bh, bl) = a, b
    return dot(jnp.concatenate([ah, al], axis=1), jnp.concatenate([bh, bh], axis=0)) + dot(ah, bl)


def start_kernel(
    sp_ref, tp_ref, fs_ref, tok_ref, gain_ref, k_ref, v_ref, q_ref, g_ref, p_ref, op_ref, od_ref,
    copies_ref, part_ref, stacked,
):
    x = tok_ref[...].astype(F32)
    scale = lax.rsqrt(jnp.mean(x * x, axis=-1, keepdims=True) + EPS)
    gain = gain_ref[...].astype(F32).reshape(1, x.shape[1])
    normed = (x * scale * gain).astype(BF16)
    for j in range(copies_ref.shape[0]):
        copies_ref[j] = normed
    f = fs_ref[0]
    depth = k_ref.shape[0]
    half = depth // 2
    rows = pl.ds(pl.multiple_of((f % 2) * half, half), half)
    part_ref[0:half] = jnp.where(f < 2, k_ref[rows, :], v_ref[rows, :])
    part_ref[half:depth] = jnp.where(f < 2, q_ref[rows, :], g_ref[rows, :])
    stacked[0:depth] = p_ref[...]
    stacked[depth : 2 * depth] = op_ref[...]
    stacked[2 * depth :] = od_ref[...]
    third = 3 * depth // 4
    part_ref[depth:] = stacked[pl.ds(pl.multiple_of(f * third, 32), third), :]


def exchange(copies, axis, groups=None):
    return lax.all_to_all(
        copies, axis, split_axis=0, concat_axis=0, tiled=True, axis_index_groups=groups
    )


def turns(x, axis, size):
    n = lax.axis_size(axis)
    out = [x]
    for d in range(1, size):
        out.append(lax.ppermute(x, axis, [(i, i - i % size + (i + d) % size) for i in range(n)]))
    return out


def gate_kernel(
    sp_ref, tp_ref, fs_ref, a_log_ref, rows_ref, tail_ref, wb_ref, wd_ref, extra_ref,
    xn_ref, beta_ref, gc_ref, decay_ref,
):
    length = rows_ref.shape[0]
    tail = tail_ref[...]
    xn_ref[0:HALO] = jnp.where(sp_ref[0] > 0, tail, jnp.zeros_like(tail))
    xn_ref[HALO:] = rows_ref[...]
    lane = tp_ref[0]

    def own_column(w_ref):
        pre = dot(rows_ref[...], w_ref[...], ((1,), (1,)))
        col = lax.broadcasted_iota(jnp.int32, pre.shape, 1)
        return jnp.sum(jnp.where(col == lane, pre, 0.0), axis=1, keepdims=True)

    beta_pre, decay_pre = own_column(wb_ref), own_column(wd_ref)
    wide = (length, 128)
    beta_ref[...] = jax.nn.sigmoid(jnp.broadcast_to(beta_pre, wide))
    rate = jnp.exp(jnp.full(wide, a_log_ref[0], F32))
    soft = jax.nn.softplus(jnp.broadcast_to(decay_pre, wide))
    extra = jnp.transpose(jnp.broadcast_to(extra_ref[...], (128, length)))
    log_gate = -rate * soft + extra
    r = lax.broadcasted_iota(jnp.int32, (length, length), 0)
    c = lax.broadcasted_iota(jnp.int32, (length, length), 1)
    lower = jnp.where(r >= c, 1.0, 0.0).astype(BF16)
    g1 = log_gate.astype(BF16)
    rest = log_gate - g1.astype(F32)
    g2 = rest.astype(BF16)
    g3 = (rest - g2.astype(F32)).astype(BF16)
    gc = dot(lower, g1) + (dot(lower, g2) + dot(lower, g3))
    gc_ref[...] = gc
    across = jnp.transpose(gc)
    across = jnp.concatenate([across] * (length // 128), axis=0)
    along = jnp.concatenate([gc] * (length // 128), axis=1)
    gaps = along - across
    decay_ref[...] = jnp.where(r >= c, jnp.exp(jnp.where(r >= c, gaps, 0.0)), 0.0)


def gather_two(f, pieces, w_scr):
    count, _, width = pieces[0].shape
    half = width // 2
    for d, piece in enumerate(pieces):
        slot = (f + 4 - d) % 4
        cols = pl.ds(pl.multiple_of((slot // 2) * width, width), width)
        for s in range(count):
            at = pl.multiple_of((2 * s + slot % 2) * half, half)
            w_scr[pl.ds(at, half), cols] = piece[s, 0:half]


def short_conv(raw, taps, length, x_scr):
    x_scr[...] = raw.astype(BF16).astype(F32)
    conv = jnp.zeros((length, raw.shape[1]), F32)
    for j in range(4):
        conv = conv + x_scr[HALO - 3 + j : HALO - 3 + j + length, :] * taps[j : j + 1, :]
    return jax.nn.silu(conv)


def unit_rows(x):
    return x * lax.rsqrt(jnp.sum(x * x, axis=-1, keepdims=True) + EPS)


def inverse_unit_lower(low, size):
    r = lax.broadcasted_iota(jnp.int32, (size, size), 0)
    c = lax.broadcasted_iota(jnp.int32, (size, size), 1)
    apart = r ^ c
    inv = [jnp.where(apart == 0, 1.0, jnp.where(apart == 1, -x, 0.0)) for x in low]
    b = 2
    while b < size:
        here = (apart >= b) & (apart < 4 * b)
        parts = [split(x) for x in inv]
        powers = [
            split(product(x, split(jnp.where(here, y, 0.0)))) for x, y in zip(parts, low)
        ]
        squares = [split(product(n, n)) for n in powers]
        inv = [x - product(n, p) for x, n, p in zip(inv, powers, parts)]
        inv = [x + product(q, split(x)) for x, q in zip(inv, squares)]
        b *= 4
    return inv


def local_kernel(
    sp_ref, tp_ref, fs_ref, xn_ref, w0_ref, w1_ref, w2_ref, w3_ref, taps_ref, beta_ref, gc_ref, decay_ref,
    ab_ref, k_ref, uw_ref,
    w_scr, k_scr, v_scr,
):
    length, width = k_ref.shape
    gather_two(fs_ref[0], (w0_ref, w1_ref, w2_ref, w3_ref), w_scr)
    raw = dot(xn_ref[...], w_scr[...])
    keys = unit_rows(short_conv(raw[:, :width], taps_ref[1], length, k_scr))
    values = short_conv(raw[:, width:], taps_ref[2], length, v_scr)
    k_ref[...] = keys
    beta = beta_ref[...]
    gc = gc_ref[...]
    kb = keys * beta
    r = lax.broadcasted_iota(jnp.int32, (length, length), 0)
    c = lax.broadcasted_iota(jnp.int32, (length, length), 1)
    corr = jnp.where(r > c, dot3(kb, keys, ((1,), (1,))) * decay_ref[...], 0.0)
    half = length // 2
    first, second = inverse_unit_lower(
        [corr[:half, :half], corr[half:, half:]], half
    )
    rhs = jnp.concatenate([values * beta, kb * jnp.exp(gc)], axis=1)
    top = dot1(first, rhs[:half])
    bottom = dot1(second, rhs[half:] - dot1(corr[half:, :half], top))
    uw_ref[0:half] = top
    uw_ref[half:] = bottom
    last = gc[length - 1 : length, :]
    kd = keys * jnp.exp(last - gc)
    made = dot1(kd, uw_ref[...], ((0,), (0,)))
    ri = lax.broadcasted_iota(jnp.int32, (width, width), 0)
    ci = lax.broadcasted_iota(jnp.int32, (width, width), 1)
    linear = jnp.where(ri == ci, jnp.exp(last), 0.0) - made[:, width:]
    ab_ref[:, :width] = linear.astype(BF16)
    ab_ref[:, width:] = made[:, :width].astype(BF16)


def step_map(later, carry, width):
    ch, cl = split(carry)
    linear = later[:, :width]
    moved = dot(linear, ch) + dot(linear, cl)
    offset = later[:, width:].astype(F32)
    return jnp.concatenate([moved[:, :width], moved[:, width:] + offset], axis=1)


def pair_map_kernel(sp_ref, tp_ref, fs_ref, own_ref, other_ref, pair_ref, before_ref):
    width = own_ref.shape[0]
    odd = sp_ref[0] % 2 == 1
    own, other = own_ref[...], other_ref[...]
    earlier = jnp.where(odd, other, own)
    later = jnp.where(odd, own, other)
    pair_ref[...] = step_map(later, earlier.astype(F32), width).astype(BF16)
    r = lax.broadcasted_iota(jnp.int32, (width, 2 * width), 0)
    c = lax.broadcasted_iota(jnp.int32, (width, 2 * width), 1)
    before_ref[...] = jnp.where(odd, other, jnp.where(r == c, 1.0, 0.0).astype(BF16))


def group_kernel(
    sp_ref, tp_ref, fs_ref, own_ref, other_ref, inner_ref,
    total_ref, linear_ref, offset_ref, before_ref,
):
    width = own_ref.shape[0]
    upper = (sp_ref[0] // 2) % 2 == 1
    own, other = own_ref[...], other_ref[...]
    earlier = jnp.where(upper, other, own)
    later = jnp.where(upper, own, other)
    total = step_map(later, earlier.astype(F32), width).astype(BF16)
    total_ref[...] = total
    linear_ref[...] = total[:, :width]
    offset_ref[...] = total[:, width:]
    inner = inner_ref[...]
    behind = step_map(inner, other.astype(F32), width)
    before_ref[...] = jnp.where(upper, behind, inner.astype(F32))


def apply(linear, state):
    high, low = split(state)
    return dot(linear, high) + dot(linear, low)


def output_kernel(
    sp_ref, tp_ref, fs_ref, xn_ref, w0_ref, w1_ref, w2_ref, w3_ref, taps_ref, gc_ref, decay_ref,
    k_ref, uw_ref, mix_ref, scale_ref, t4_ref, a8_ref, b8_ref, b12_ref, before_ref, gain_ref,
    mine_ref, other_ref,
    w_scr, w_all, q_scr, a_scr, b_scr,
):
    length, width = k_ref.shape
    pieces = (w0_ref, w1_ref, w2_ref, w3_ref)
    state = apply(a8_ref[...], b12_ref[...].astype(F32)) + b8_ref[...].astype(F32)
    state = apply(t4_ref[:, :width], state) + t4_ref[:, width:].astype(F32)
    state = dot3(before_ref[:, :width], state) + before_ref[:, width:]
    gather_two(fs_ref[0], pieces, w_scr)
    count, part, _ = w0_ref.shape
    skip = width // 2
    part = part - skip
    for d, piece in enumerate(pieces):
        at = pl.multiple_of(((fs_ref[0] + 4 - d) % 4) * part, 32)
        for s in range(count):
            w_all[pl.ds(at, part), s * width : (s + 1) * width] = piece[s, skip:]
    for s in range(count):
        w_scr[s * width : (s + 1) * width, 2 * width :] = w_all[
            0:width, s * width : (s + 1) * width
        ]
    raw = dot(xn_ref[...], w_scr[...])
    query = unit_rows(short_conv(raw[:, :width], taps_ref[0], length, q_scr)) * width ** (-0.5)
    silu_gate = jax.nn.silu(raw[HALO:, width : 2 * width].astype(BF16).astype(F32))
    scores = dot1(query, k_ref[...], ((1,), (1,))) * decay_ref[...]
    both = dot1(scores, uw_ref[...])
    effect = query * jnp.exp(gc_ref[...]) - both[:, width:]
    attended = both[:, :width] + dot1(effect, state)
    scale = lax.rsqrt(jnp.mean(attended * attended, axis=-1, keepdims=True) + EPS)
    delta = (attended * scale * gain_ref[...] * silu_gate).astype(BF16)
    x = raw[:, 2 * width :].astype(BF16).astype(F32)
    kind = tp_ref[0] % 4
    total = HALO + length
    a_scr[0:HALO] = jnp.zeros((HALO, width), F32)
    b_scr[0:HALO] = jnp.zeros((HALO, width), F32)
    a_scr[HALO:] = x
    two = x + a_scr[HALO - 1 : HALO - 1 + total]
    b_scr[HALO:] = two
    four = two + b_scr[HALO - 2 : HALO - 2 + total]
    a_scr[HALO:] = four
    eight = four + a_scr[HALO - 4 : HALO - 4 + total]
    b_scr[HALO:] = eight
    sixteen = eight + b_scr[HALO - 8 : HALO - 8 + total]
    window = jnp.where(
        kind == 0, two, jnp.where(kind == 1, four, jnp.where(kind == 2, eight, sixteen))
    )
    window = window[HALO:]
    place = sp_ref[0] * length + lax.broadcasted_iota(jnp.int32, (length, width), 0)
    span = jnp.where(kind == 0, 2, jnp.where(kind == 1, 4, jnp.where(kind == 2, 8, 16)))
    counts = jnp.minimum(place + 1, span).astype(F32)
    pooled = (window / counts - x[HALO:]).astype(BF16)
    pool_out = (dot(pooled, mix_ref[...]) * scale_ref[...]).astype(BF16)
    channels = jnp.concatenate([pool_out, delta], axis=1)
    core = tp_ref[0] % 2
    chips, rows, cols = mine_ref.shape
    step = 512
    for at in range(0, cols, step):
        made = dot(channels, w_all[width:, at : at + step]).astype(BF16)
        for j in range(chips):
            even = made[2 * j * rows : (2 * j + 1) * rows]
            odd = made[(2 * j + 1) * rows : (2 * j + 2) * rows]
            mine_ref[j, :, at : at + step] = jnp.where(core == 0, even, odd)
            other_ref[j, :, at : at + step] = jnp.where(core == 0, odd, even)


def pair_kernel(mine_ref, theirs_ref, out_ref):
    out_ref[...] = (mine_ref[...].astype(F32) + theirs_ref[...].astype(F32)).astype(BF16)


def sum_kernel(in_ref, out_ref):
    total = in_ref[0].astype(F32)
    for j in range(1, in_ref.shape[0]):
        total = total + in_ref[j].astype(F32)
    out_ref[...] = total.astype(BF16)


def layer(
    tokens,
    norm_gain,
    w_pool_in,
    w_query,
    w_key,
    w_value,
    w_gate,
    w_beta,
    w_decay,
    conv_weight,
    a_log,
    decay_extra,
    w_mix,
    pool_scale,
    delta_gain,
    w_out_pool,
    w_out_delta,
):
    n_sp = lax.axis_size("sp")
    n_tp = lax.axis_size("tp")
    sp_id = lax.axis_index("sp").astype(jnp.int32)
    tp_id = lax.axis_index("tp").astype(jnp.int32)
    fs_id = lax.axis_index("fs").astype(jnp.int32)
    ids = (sp_id[None], tp_id[None], fs_id[None])
    depth, width = w_key.shape
    rows, model = tokens.shape
    length = rows * n_tp
    half = depth // 2

    copies, part = call(
        start_kernel,
        (shape(n_tp, rows, model, dtype=BF16), shape(7 * depth // 4, width, dtype=BF16)),
        *ids, tokens, norm_gain,
        w_key, w_value, w_query, w_gate, w_pool_in, w_out_pool, w_out_delta,
        scratch=[pltpu.VMEM((3 * depth, width), BF16)], vmem=None,
    )
    all_rows = exchange(copies, "tp").reshape(length, model)
    tail = lax.ppermute(
        all_rows[length - HALO :], "sp", [(i, i + 1) for i in range(n_sp - 1)]
    )
    quarters = lax.all_gather(part, "sp", axis=0)
    kv = turns(quarters[:, :half], "fs", 4)
    rest = turns(quarters[:, half:], "fs", 4)

    xn, beta, gc, decay = call(
        gate_kernel,
        (
            shape(HALO + length, model, dtype=BF16),
            shape(length, 128),
            shape(length, 128),
            shape(length, length),
        ),
        *ids, a_log, all_rows, tail, w_beta.T, w_decay.T, decay_extra.T,
        smem=4, flops=2 * length * model * 128,
    )
    ab, keys, uw = call(
        local_kernel,
        (shape(width, 2 * width, dtype=BF16), shape(length, width), shape(length, 2 * width)),
        *ids, xn, *kv, conv_weight, beta, gc, decay,
        scratch=[
            pltpu.VMEM((model, 2 * width), BF16),
            pltpu.VMEM((HALO + length, width), F32),
            pltpu.VMEM((HALO + length, width), F32),
        ],
        flops=20 * length * model * width,
    )
    quad = 4

    def meet(x, distance):
        return lax.ppermute(x, "sp", [(i, i ^ distance) for i in range(n_sp)])

    pair, inner = call(
        pair_map_kernel,
        (shape(width, 2 * width, dtype=BF16), shape(width, 2 * width, dtype=BF16)),
        *ids, ab, meet(ab, 1),
        flops=20 * width**3,
    )
    total, linear, offset, before = call(
        group_kernel,
        (
            shape(width, 2 * width, dtype=BF16),
            shape(width, width, dtype=BF16),
            shape(width, width, dtype=BF16),
            shape(width, 2 * width),
        ),
        *ids, pair, meet(pair, 2), inner,
        flops=20 * width**3,
    )

    def from_behind(x, first, last, distance):
        return lax.ppermute(x, "sp", [(i, i + distance) for i in range(first, last)])

    t4 = from_behind(total, 0, n_sp - quad, quad)
    b8 = from_behind(offset, 0, n_sp - 2 * quad, 2 * quad)
    a8 = from_behind(linear, quad, n_sp - 2 * quad, 2 * quad)
    b12 = from_behind(offset, 0, n_sp - 3 * quad, 3 * quad)

    chips = n_tp // 2
    mine, other = call(
        output_kernel,
        (shape(chips, rows, model, dtype=BF16), shape(chips, rows, model, dtype=BF16)),
        *ids, xn, *rest, conv_weight, gc, decay, keys, uw, w_mix[0], pool_scale.reshape(1, width),
        t4, a8, b8, b12, before, delta_gain.reshape(1, width),
        scratch=[
            pltpu.VMEM((model, 3 * width), BF16),
            pltpu.VMEM((3 * width, model), BF16),
            pltpu.VMEM((HALO + length, width), F32),
            pltpu.VMEM((2 * HALO + length, width), F32),
            pltpu.VMEM((2 * HALO + length, width), F32),
        ],
        flops=20 * length * model * width,
    )
    theirs = lax.ppermute(other, "tp", [(i, i ^ 1) for i in range(n_tp)])
    partial = call(
        pair_kernel, shape(chips, rows, model, dtype=BF16), mine, theirs, smem=0, flops=1000000
    )
    cores = [[2 * x + c for x in range(chips)] for c in range(2)]
    arrived = exchange(partial, "tp", cores)
    return call(sum_kernel, shape(rows, model, dtype=BF16), arrived, smem=0, flops=1000000)


def solution(mesh):
    placed = (
        P(("fs", "sp", "tp"), None),
        P(),
        P("sp", "tp"),
        P("sp", "tp"),
        P("sp", "tp"),
        P("sp", "tp"),
        P("sp", "tp"),
        P(),
        P(),
        P(None, None, "tp"),
        P("tp"),
        P(("fs", "sp"), "tp"),
        P("tp", None, None),
        P("tp"),
        P(),
        P("tp", "sp"),
        P("tp", "sp"),
    )
    return jax.shard_map(
        layer,
        mesh=mesh,
        in_specs=placed,
        out_specs=P(("fs", "sp", "tp"), None),
        check_vma=False,
    )
```

```python
import jax
import jax.numpy as jnp
from jax import lax
from jax.experimental import pallas as pl
from jax.experimental.pallas import tpu as pltpu
from jax.sharding import PartitionSpec as P


EPS = 1e-06
HALO = 16
F32 = jnp.float32
BF16 = jnp.bfloat16


def call(kernel, outs, *args, smem=3, scratch=(), flops=0, vmem=16):
    in_specs = [pl.BlockSpec(memory_space=pltpu.SMEM)] * smem + [
        pl.BlockSpec(memory_space=pltpu.VMEM)
    ] * (len(args) - smem)
    many = isinstance(outs, (list, tuple))
    out_specs = pl.BlockSpec(memory_space=pltpu.VMEM)
    return pl.pallas_call(
        kernel,
        out_shape=list(outs) if many else outs,
        in_specs=in_specs,
        out_specs=[out_specs] * len(outs) if many else out_specs,
        scratch_shapes=list(scratch),
        compiler_params=pltpu.CompilerParams(vmem_limit_bytes=vmem and vmem * 1024 * 1024),
        cost_estimate=pl.CostEstimate(flops=flops, bytes_accessed=0, transcendentals=0),
    )(*args)


def shape(*dims, dtype=F32):
    return jax.ShapeDtypeStruct(dims, dtype)


def dot(a, b, dims=((1,), (0,))):
    return lax.dot_general(a, b, (dims, ((), ())), preferred_element_type=F32)


def split(a):
    high = a.astype(BF16)
    return high, (a - high.astype(F32)).astype(BF16)


def dot1(a, b, dims=((1,), (0,))):
    return dot(a.astype(BF16), b.astype(BF16), dims)


def dot3(a, b, dims=((1,), (0,))):
    ah, al = split(a)
    bh, bl = split(b)
    return dot(ah, bh, dims) + (dot(ah, bl, dims) + dot(al, bh, dims))


def product(a, b):
    (ah, al), (bh, bl) = a, b
    return dot(jnp.concatenate([ah, al], axis=1), jnp.concatenate([bh, bh], axis=0)) + dot(ah, bl)


def start_kernel(
    sp_ref, tp_ref, fs_ref, tok_ref, gain_ref, k_ref, v_ref, q_ref, g_ref, p_ref, op_ref, od_ref,
    copies_ref, part_ref, stacked,
):
    x = tok_ref[...].astype(F32)
    scale = lax.rsqrt(jnp.mean(x * x, axis=-1, keepdims=True) + EPS)
    gain = gain_ref[...].astype(F32).reshape(1, x.shape[1])
    normed = (x * scale * gain).astype(BF16)
    for j in range(copies_ref.shape[0]):
        copies_ref[j] = normed
    f = fs_ref[0]
    depth = k_ref.shape[0]
    half = depth // 2
    rows = pl.ds(pl.multiple_of((f % 2) * half, half), half)
    part_ref[0:half] = jnp.where(f < 2, k_ref[rows, :], v_ref[rows, :])
    part_ref[half:depth] = jnp.where(f < 2, q_ref[rows, :], g_ref[rows, :])
    stacked[0:depth] = p_ref[...]
    stacked[depth : 2 * depth] = op_ref[...]
    stacked[2 * depth :] = od_ref[...]
    third = 3 * depth // 4
    part_ref[depth:] = stacked[pl.ds(pl.multiple_of(f * third, 32), third), :]


def exchange(copies, axis, groups=None):
    return lax.all_to_all(
        copies, axis, split_axis=0, concat_axis=0, tiled=True, axis_index_groups=groups
    )


def turns(x, axis, size):
    n = lax.axis_size(axis)
    out = [x]
    for d in range(1, size):
        out.append(lax.ppermute(x, axis, [(i, i - i % size + (i + d) % size) for i in range(n)]))
    return out


def gate_kernel(
    sp_ref, tp_ref, fs_ref, a_log_ref, rows_ref, wb_ref, wd_ref, extra_ref,
    beta_ref, gc_ref, decay_ref,
):
    length = rows_ref.shape[0]
    lane = tp_ref[0]

    def own_column(w_ref):
        pre = dot(rows_ref[...], w_ref[...], ((1,), (1,)))
        col = lax.broadcasted_iota(jnp.int32, pre.shape, 1)
        return jnp.sum(jnp.where(col == lane, pre, 0.0), axis=1, keepdims=True)

    beta_pre, decay_pre = own_column(wb_ref), own_column(wd_ref)
    wide = (length, 128)
    beta_ref[...] = jax.nn.sigmoid(jnp.broadcast_to(beta_pre, wide))
    rate = jnp.exp(jnp.full(wide, a_log_ref[0], F32))
    soft = jax.nn.softplus(jnp.broadcast_to(decay_pre, wide))
    extra = jnp.transpose(jnp.broadcast_to(extra_ref[...], (128, length)))
    log_gate = -rate * soft + extra
    r = lax.broadcasted_iota(jnp.int32, (length, length), 0)
    c = lax.broadcasted_iota(jnp.int32, (length, length), 1)
    lower = jnp.where(r >= c, 1.0, 0.0).astype(BF16)
    g1 = log_gate.astype(BF16)
    rest = log_gate - g1.astype(F32)
    g2 = rest.astype(BF16)
    g3 = (rest - g2.astype(F32)).astype(BF16)
    gc = dot(lower, g1) + (dot(lower, g2) + dot(lower, g3))
    gc_ref[...] = gc
    across = jnp.transpose(gc)
    across = jnp.concatenate([across] * (length // 128), axis=0)
    along = jnp.concatenate([gc] * (length // 128), axis=1)
    gaps = along - across
    decay_ref[...] = jnp.where(r >= c, jnp.exp(jnp.where(r >= c, gaps, 0.0)), 0.0)


def gather_two(f, pieces, w_scr):
    count, _, width = pieces[0].shape
    half = width // 2
    for d, piece in enumerate(pieces):
        slot = (f + 4 - d) % 4
        cols = pl.ds(pl.multiple_of((slot // 2) * width, width), width)
        for s in range(count):
            at = pl.multiple_of((2 * s + slot % 2) * half, half)
            w_scr[pl.ds(at, half), cols] = piece[s, 0:half]


def short_conv(raw, taps, length, x_scr):
    x_scr[...] = raw.astype(BF16).astype(F32)
    conv = jnp.zeros((length, raw.shape[1]), F32)
    for j in range(4):
        conv = conv + x_scr[HALO - 3 + j : HALO - 3 + j + length, :] * taps[j : j + 1, :]
    return jax.nn.silu(conv)


def unit_rows(x):
    return x * lax.rsqrt(jnp.sum(x * x, axis=-1, keepdims=True) + EPS)


def inverse_unit_lower(low, size):
    r = lax.broadcasted_iota(jnp.int32, (size, size), 0)
    c = lax.broadcasted_iota(jnp.int32, (size, size), 1)
    apart = r ^ c
    inv = [jnp.where(apart == 0, 1.0, jnp.where(apart == 1, -x, 0.0)) for x in low]
    b = 2
    while b < size:
        here = (apart >= b) & (apart < 4 * b)
        parts = [split(x) for x in inv]
        powers = [
            split(product(x, split(jnp.where(here, y, 0.0)))) for x, y in zip(parts, low)
        ]
        squares = [split(product(n, n)) for n in powers]
        inv = [x - product(n, p) for x, n, p in zip(inv, powers, parts)]
        inv = [x + product(q, split(x)) for x, q in zip(inv, squares)]
        b *= 4
    return inv


def local_kernel(
    sp_ref, tp_ref, fs_ref, rows_ref, tail_ref, w0_ref, w1_ref, w2_ref, w3_ref, taps_ref,
    beta_ref, gc_ref, decay_ref,
    ab_ref, k_ref, uw_ref, xn_ref,
    w_scr, k_scr, v_scr,
):
    length, width = k_ref.shape
    tail = tail_ref[...]
    xn_ref[0:HALO] = jnp.where(sp_ref[0] > 0, tail, jnp.zeros_like(tail))
    xn_ref[HALO:] = rows_ref[...]
    gather_two(fs_ref[0], (w0_ref, w1_ref, w2_ref, w3_ref), w_scr)
    raw = dot(xn_ref[...], w_scr[...])
    keys = unit_rows(short_conv(raw[:, :width], taps_ref[1], length, k_scr))
    values = short_conv(raw[:, width:], taps_ref[2], length, v_scr)
    k_ref[...] = keys
    beta = beta_ref[...]
    gc = gc_ref[...]
    kb = keys * beta
    r = lax.broadcasted_iota(jnp.int32, (length, length), 0)
    c = lax.broadcasted_iota(jnp.int32, (length, length), 1)
    corr = jnp.where(r > c, dot3(kb, keys, ((1,), (1,))) * decay_ref[...], 0.0)
    half = length // 2
    first, second = inverse_unit_lower(
        [corr[:half, :half], corr[half:, half:]], half
    )
    rhs = jnp.concatenate([values * beta, kb * jnp.exp(gc)], axis=1)
    top = dot1(first, rhs[:half])
    bottom = dot1(second, rhs[half:] - dot1(corr[half:, :half], top))
    uw_ref[0:half] = top
    uw_ref[half:] = bottom
    last = gc[length - 1 : length, :]
    kd = keys * jnp.exp(last - gc)
    made = dot1(kd, uw_ref[...], ((0,), (0,)))
    ri = lax.broadcasted_iota(jnp.int32, (width, width), 0)
    ci = lax.broadcasted_iota(jnp.int32, (width, width), 1)
    linear = jnp.where(ri == ci, jnp.exp(last), 0.0) - made[:, width:]
    ab_ref[:, :width] = linear.astype(BF16)
    ab_ref[:, width:] = made[:, :width].astype(BF16)


def step_map(later, carry, width):
    ch, cl = split(carry)
    linear = later[:, :width]
    moved = dot(linear, ch) + dot(linear, cl)
    offset = later[:, width:].astype(F32)
    return jnp.concatenate([moved[:, :width], moved[:, width:] + offset], axis=1)


def pair_map_kernel(sp_ref, tp_ref, fs_ref, own_ref, other_ref, pair_ref, before_ref):
    width = own_ref.shape[0]
    odd = sp_ref[0] % 2 == 1
    own, other = own_ref[...], other_ref[...]
    earlier = jnp.where(odd, other, own)
    later = jnp.where(odd, own, other)
    pair_ref[...] = step_map(later, earlier.astype(F32), width).astype(BF16)
    r = lax.broadcasted_iota(jnp.int32, (width, 2 * width), 0)
    c = lax.broadcasted_iota(jnp.int32, (width, 2 * width), 1)
    before_ref[...] = jnp.where(odd, other, jnp.where(r == c, 1.0, 0.0).astype(BF16))


def group_kernel(
    sp_ref, tp_ref, fs_ref, own_ref, other_ref, inner_ref,
    total_ref, linear_ref, offset_ref, before_ref,
):
    width = own_ref.shape[0]
    upper = (sp_ref[0] // 2) % 2 == 1
    own, other = own_ref[...], other_ref[...]
    earlier = jnp.where(upper, other, own)
    later = jnp.where(upper, own, other)
    total = step_map(later, earlier.astype(F32), width).astype(BF16)
    total_ref[...] = total
    linear_ref[...] = total[:, :width]
    offset_ref[...] = total[:, width:]
    inner = inner_ref[...]
    behind = step_map(inner, other.astype(F32), width)
    before_ref[...] = jnp.where(upper, behind, inner.astype(F32))


def apply(linear, state):
    high, low = split(state)
    return dot(linear, high) + dot(linear, low)


def output_kernel(
    sp_ref, tp_ref, fs_ref, xn_ref, w0_ref, w1_ref, w2_ref, w3_ref, taps_ref, gc_ref, decay_ref,
    k_ref, uw_ref, mix_ref, scale_ref, t4_ref, a8_ref, b8_ref, b12_ref, before_ref, gain_ref,
    mine_ref, other_ref,
    w_scr, w_all, q_scr, a_scr, b_scr,
):
    length, width = k_ref.shape
    pieces = (w0_ref, w1_ref, w2_ref, w3_ref)
    state = apply(a8_ref[...], b12_ref[...].astype(F32)) + b8_ref[...].astype(F32)
    state = apply(t4_ref[:, :width], state) + t4_ref[:, width:].astype(F32)
    state = dot3(before_ref[:, :width], state) + before_ref[:, width:]
    gather_two(fs_ref[0], pieces, w_scr)
    count, part, _ = w0_ref.shape
    skip = width // 2
    part = part - skip
    for d, piece in enumerate(pieces):
        at = pl.multiple_of(((fs_ref[0] + 4 - d) % 4) * part, 32)
        for s in range(count):
            w_all[pl.ds(at, part), s * width : (s + 1) * width] = piece[s, skip:]
    for s in range(count):
        w_scr[s * width : (s + 1) * width, 2 * width :] = w_all[
            0:width, s * width : (s + 1) * width
        ]
    raw = dot(xn_ref[...], w_scr[...])
    query = unit_rows(short_conv(raw[:, :width], taps_ref[0], length, q_scr)) * width ** (-0.5)
    silu_gate = jax.nn.silu(raw[HALO:, width : 2 * width].astype(BF16).astype(F32))
    scores = dot1(query, k_ref[...], ((1,), (1,))) * decay_ref[...]
    both = dot1(scores, uw_ref[...])
    effect = query * jnp.exp(gc_ref[...]) - both[:, width:]
    attended = both[:, :width] + dot1(effect, state)
    scale = lax.rsqrt(jnp.mean(attended * attended, axis=-1, keepdims=True) + EPS)
    delta = (attended * scale * gain_ref[...] * silu_gate).astype(BF16)
    x = raw[:, 2 * width :].astype(BF16).astype(F32)
    kind = tp_ref[0] % 4
    total = HALO + length
    a_scr[0:HALO] = jnp.zeros((HALO, width), F32)
    b_scr[0:HALO] = jnp.zeros((HALO, width), F32)
    a_scr[HALO:] = x
    two = x + a_scr[HALO - 1 : HALO - 1 + total]
    b_scr[HALO:] = two
    four = two + b_scr[HALO - 2 : HALO - 2 + total]
    a_scr[HALO:] = four
    eight = four + a_scr[HALO - 4 : HALO - 4 + total]
    b_scr[HALO:] = eight
    sixteen = eight + b_scr[HALO - 8 : HALO - 8 + total]
    window = jnp.where(
        kind == 0, two, jnp.where(kind == 1, four, jnp.where(kind == 2, eight, sixteen))
    )
    window = window[HALO:]
    place = sp_ref[0] * length + lax.broadcasted_iota(jnp.int32, (length, width), 0)
    span = jnp.where(kind == 0, 2, jnp.where(kind == 1, 4, jnp.where(kind == 2, 8, 16)))
    counts = jnp.minimum(place + 1, span).astype(F32)
    pooled = (window / counts - x[HALO:]).astype(BF16)
    pool_out = (dot(pooled, mix_ref[...]) * scale_ref[...]).astype(BF16)
    channels = jnp.concatenate([pool_out, delta], axis=1)
    core = tp_ref[0] % 2
    chips, rows, cols = mine_ref.shape
    step = 512
    for at in range(0, cols, step):
        made = dot(channels, w_all[width:, at : at + step]).astype(BF16)
        for j in range(chips):
            even = made[2 * j * rows : (2 * j + 1) * rows]
            odd = made[(2 * j + 1) * rows : (2 * j + 2) * rows]
            mine_ref[j, :, at : at + step] = jnp.where(core == 0, even, odd)
            other_ref[j, :, at : at + step] = jnp.where(core == 0, odd, even)


def pair_kernel(mine_ref, theirs_ref, out_ref):
    out_ref[...] = (mine_ref[...].astype(F32) + theirs_ref[...].astype(F32)).astype(BF16)


def sum_kernel(in_ref, out_ref):
    total = in_ref[0].astype(F32)
    for j in range(1, in_ref.shape[0]):
        total = total + in_ref[j].astype(F32)
    out_ref[...] = total.astype(BF16)


def layer(
    tokens,
    norm_gain,
    w_pool_in,
    w_query,
    w_key,
    w_value,
    w_gate,
    w_beta,
    w_decay,
    conv_weight,
    a_log,
    decay_extra,
    w_mix,
    pool_scale,
    delta_gain,
    w_out_pool,
    w_out_delta,
):
    n_sp = lax.axis_size("sp")
    n_tp = lax.axis_size("tp")
    sp_id = lax.axis_index("sp").astype(jnp.int32)
    tp_id = lax.axis_index("tp").astype(jnp.int32)
    fs_id = lax.axis_index("fs").astype(jnp.int32)
    ids = (sp_id[None], tp_id[None], fs_id[None])
    depth, width = w_key.shape
    rows, model = tokens.shape
    length = rows * n_tp
    half = depth // 2

    copies, part = call(
        start_kernel,
        (shape(n_tp, rows, model, dtype=BF16), shape(7 * depth // 4, width, dtype=BF16)),
        *ids, tokens, norm_gain,
        w_key, w_value, w_query, w_gate, w_pool_in, w_out_pool, w_out_delta,
        scratch=[pltpu.VMEM((3 * depth, width), BF16)], vmem=None,
    )
    all_rows = exchange(copies, "tp").reshape(length, model)
    tail = lax.ppermute(
        all_rows[length - HALO :], "sp", [(i, i + 1) for i in range(n_sp - 1)]
    )
    quarters = lax.all_gather(part, "sp", axis=0)
    kv = turns(quarters[:, :half], "fs", 4)
    rest = turns(quarters[:, half:], "fs", 4)

    beta, gc, decay = call(
        gate_kernel,
        (
            shape(length, 128),
            shape(length, 128),
            shape(length, length),
        ),
        *ids, a_log, all_rows, w_beta.T, w_decay.T, decay_extra.T,
        smem=4, flops=2 * length * model * 128,
    )
    ab, keys, uw, xn = call(
        local_kernel,
        (
            shape(width, 2 * width, dtype=BF16),
            shape(length, width),
            shape(length, 2 * width),
            shape(HALO + length, model, dtype=BF16),
        ),
        *ids, all_rows, tail, *kv, conv_weight, beta, gc, decay,
        scratch=[
            pltpu.VMEM((model, 2 * width), BF16),
            pltpu.VMEM((HALO + length, width), F32),
            pltpu.VMEM((HALO + length, width), F32),
        ],
        flops=20 * length * model * width,
    )
    quad = 4

    def meet(x, distance):
        return lax.ppermute(x, "sp", [(i, i ^ distance) for i in range(n_sp)])

    pair, inner = call(
        pair_map_kernel,
        (shape(width, 2 * width, dtype=BF16), shape(width, 2 * width, dtype=BF16)),
        *ids, ab, meet(ab, 1),
        flops=20 * width**3,
    )
    total, linear, offset, before = call(
        group_kernel,
        (
            shape(width, 2 * width, dtype=BF16),
            shape(width, width, dtype=BF16),
            shape(width, width, dtype=BF16),
            shape(width, 2 * width),
        ),
        *ids, pair, meet(pair, 2), inner,
        flops=20 * width**3,
    )

    def from_behind(x, first, last, distance):
        return lax.ppermute(x, "sp", [(i, i + distance) for i in range(first, last)])

    t4 = from_behind(total, 0, n_sp - quad, quad)
    b8 = from_behind(offset, 0, n_sp - 2 * quad, 2 * quad)
    a8 = from_behind(linear, quad, n_sp - 2 * quad, 2 * quad)
    b12 = from_behind(offset, 0, n_sp - 3 * quad, 3 * quad)

    chips = n_tp // 2
    mine, other = call(
        output_kernel,
        (shape(chips, rows, model, dtype=BF16), shape(chips, rows, model, dtype=BF16)),
        *ids, xn, *rest, conv_weight, gc, decay, keys, uw, w_mix[0], pool_scale.reshape(1, width),
        t4, a8, b8, b12, before, delta_gain.reshape(1, width),
        scratch=[
            pltpu.VMEM((model, 3 * width), BF16),
            pltpu.VMEM((3 * width, model), BF16),
            pltpu.VMEM((HALO + length, width), F32),
            pltpu.VMEM((2 * HALO + length, width), F32),
            pltpu.VMEM((2 * HALO + length, width), F32),
        ],
        flops=20 * length * model * width,
    )
    theirs = lax.ppermute(other, "tp", [(i, i ^ 1) for i in range(n_tp)])
    partial = call(
        pair_kernel, shape(chips, rows, model, dtype=BF16), mine, theirs, smem=0, flops=1000000
    )
    cores = [[2 * x + c for x in range(chips)] for c in range(2)]
    arrived = exchange(partial, "tp", cores)
    return call(sum_kernel, shape(rows, model, dtype=BF16), arrived, smem=0, flops=1000000)


def solution(mesh):
    placed = (
        P(("fs", "sp", "tp"), None),
        P(),
        P("sp", "tp"),
        P("sp", "tp"),
        P("sp", "tp"),
        P("sp", "tp"),
        P("sp", "tp"),
        P(),
        P(),
        P(None, None, "tp"),
        P("tp"),
        P(("fs", "sp"), "tp"),
        P("tp", None, None),
        P("tp"),
        P(),
        P("tp", "sp"),
        P("tp", "sp"),
    )
    return jax.shard_map(
        layer,
        mesh=mesh,
        in_specs=placed,
        out_specs=P(("fs", "sp", "tp"), None),
        check_vma=False,
    )
```

```python
import jax
import jax.numpy as jnp
from jax import lax
from jax.experimental import pallas as pl
from jax.experimental.pallas import tpu as pltpu
from jax.sharding import PartitionSpec as P


EPS = 1e-06
HALO = 16
F32 = jnp.float32
BF16 = jnp.bfloat16


def call(kernel, outs, *args, smem=3, scratch=(), flops=0, vmem=16):
    in_specs = [pl.BlockSpec(memory_space=pltpu.SMEM)] * smem + [
        pl.BlockSpec(memory_space=pltpu.VMEM)
    ] * (len(args) - smem)
    many = isinstance(outs, (list, tuple))
    out_specs = pl.BlockSpec(memory_space=pltpu.VMEM)
    return pl.pallas_call(
        kernel,
        out_shape=list(outs) if many else outs,
        in_specs=in_specs,
        out_specs=[out_specs] * len(outs) if many else out_specs,
        scratch_shapes=list(scratch),
        compiler_params=pltpu.CompilerParams(vmem_limit_bytes=vmem and vmem * 1024 * 1024),
        cost_estimate=pl.CostEstimate(flops=flops, bytes_accessed=0, transcendentals=0),
    )(*args)


def shape(*dims, dtype=F32):
    return jax.ShapeDtypeStruct(dims, dtype)


def dot(a, b, dims=((1,), (0,))):
    return lax.dot_general(a, b, (dims, ((), ())), preferred_element_type=F32)


def split(a):
    high = a.astype(BF16)
    return high, (a - high.astype(F32)).astype(BF16)


def dot1(a, b, dims=((1,), (0,))):
    return dot(a.astype(BF16), b.astype(BF16), dims)


def dot3(a, b, dims=((1,), (0,))):
    ah, al = split(a)
    bh, bl = split(b)
    return dot(ah, bh, dims) + (dot(ah, bl, dims) + dot(al, bh, dims))


def product(a, b):
    (ah, al), (bh, bl) = a, b
    return dot(jnp.concatenate([ah, al], axis=1), jnp.concatenate([bh, bh], axis=0)) + dot(ah, bl)


def start_kernel(
    sp_ref, tp_ref, fs_ref, tok_ref, gain_ref, k_ref, v_ref, q_ref, g_ref, p_ref, op_ref, od_ref,
    copies_ref, part_ref, stacked,
):
    x = tok_ref[...].astype(F32)
    scale = lax.rsqrt(jnp.mean(x * x, axis=-1, keepdims=True) + EPS)
    gain = gain_ref[...].astype(F32).reshape(1, x.shape[1])
    normed = (x * scale * gain).astype(BF16)
    for j in range(copies_ref.shape[0]):
        copies_ref[j] = normed
    f = fs_ref[0]
    depth = k_ref.shape[0]
    half = depth // 2
    rows = pl.ds(pl.multiple_of((f % 2) * half, half), half)
    part_ref[0:half] = jnp.where(f < 2, k_ref[rows, :], v_ref[rows, :])
    part_ref[half:depth] = jnp.where(f < 2, q_ref[rows, :], g_ref[rows, :])
    stacked[0:depth] = p_ref[...]
    stacked[depth : 2 * depth] = op_ref[...]
    stacked[2 * depth :] = od_ref[...]
    third = 3 * depth // 4
    part_ref[depth:] = stacked[pl.ds(pl.multiple_of(f * third, 32), third), :]


def exchange(copies, axis, groups=None):
    return lax.all_to_all(
        copies, axis, split_axis=0, concat_axis=0, tiled=True, axis_index_groups=groups
    )


def turns(x, axis, size):
    n = lax.axis_size(axis)
    out = [x]
    for d in range(1, size):
        out.append(lax.ppermute(x, axis, [(i, i - i % size + (i + d) % size) for i in range(n)]))
    return out


def gate_kernel(
    sp_ref, tp_ref, fs_ref, a_log_ref, rows_ref, wb_ref, wd_ref, extra_ref,
    beta_ref, gc_ref, decay_ref,
):
    length = rows_ref.shape[0]
    lane = tp_ref[0]

    def own_column(w_ref):
        pre = dot(rows_ref[...], w_ref[...], ((1,), (1,)))
        col = lax.broadcasted_iota(jnp.int32, pre.shape, 1)
        return jnp.sum(jnp.where(col == lane, pre, 0.0), axis=1, keepdims=True)

    beta_pre, decay_pre = own_column(wb_ref), own_column(wd_ref)
    wide = (length, 128)
    beta_ref[...] = jax.nn.sigmoid(jnp.broadcast_to(beta_pre, wide))
    rate = jnp.exp(jnp.full(wide, a_log_ref[0], F32))
    soft = jax.nn.softplus(jnp.broadcast_to(decay_pre, wide))
    extra = jnp.transpose(jnp.broadcast_to(extra_ref[...], (128, length)))
    log_gate = -rate * soft + extra
    r = lax.broadcasted_iota(jnp.int32, (length, length), 0)
    c = lax.broadcasted_iota(jnp.int32, (length, length), 1)
    lower = jnp.where(r >= c, 1.0, 0.0).astype(BF16)
    g1 = log_gate.astype(BF16)
    rest = log_gate - g1.astype(F32)
    g2 = rest.astype(BF16)
    g3 = (rest - g2.astype(F32)).astype(BF16)
    gc = dot(lower, g1) + (dot(lower, g2) + dot(lower, g3))
    gc_ref[...] = gc
    across = jnp.transpose(gc)
    across = jnp.concatenate([across] * (length // 128), axis=0)
    along = jnp.concatenate([gc] * (length // 128), axis=1)
    gaps = along - across
    decay_ref[...] = jnp.where(r >= c, jnp.exp(jnp.where(r >= c, gaps, 0.0)), 0.0)


def gather_two(f, pieces, w_scr):
    count, _, width = pieces[0].shape
    half = width // 2
    for d, piece in enumerate(pieces):
        slot = (f + 4 - d) % 4
        cols = pl.ds(pl.multiple_of((slot // 2) * width, width), width)
        for s in range(count):
            at = pl.multiple_of((2 * s + slot % 2) * half, half)
            w_scr[pl.ds(at, half), cols] = piece[s, 0:half]


def short_conv(raw, taps, length, x_scr):
    x_scr[...] = raw.astype(BF16).astype(F32)
    conv = jnp.zeros((length, raw.shape[1]), F32)
    for j in range(4):
        conv = conv + x_scr[HALO - 3 + j : HALO - 3 + j + length, :] * taps[j : j + 1, :]
    return jax.nn.silu(conv)


def unit_rows(x):
    return x * lax.rsqrt(jnp.sum(x * x, axis=-1, keepdims=True) + EPS)


def inverse_unit_lower(low, size):
    r = lax.broadcasted_iota(jnp.int32, (size, size), 0)
    c = lax.broadcasted_iota(jnp.int32, (size, size), 1)
    apart = r ^ c
    inv = [jnp.where(apart == 0, 1.0, jnp.where(apart == 1, -x, 0.0)) for x in low]
    b = 2
    while b < size:
        here = (apart >= b) & (apart < 4 * b)
        parts = [split(x) for x in inv]
        powers = [
            split(product(x, split(jnp.where(here, y, 0.0)))) for x, y in zip(parts, low)
        ]
        squares = [split(product(n, n)) for n in powers]
        inv = [x - product(n, p) for x, n, p in zip(inv, powers, parts)]
        inv = [x + product(q, split(x)) for x, q in zip(inv, squares)]
        b *= 4
    return inv


def local_kernel(
    sp_ref, tp_ref, fs_ref, rows_ref, tail_ref, w0_ref, w1_ref, w2_ref, w3_ref, taps_ref,
    beta_ref, gc_ref, decay_ref,
    ab_ref, k_ref, uw_ref, xn_ref,
    w_scr, k_scr, v_scr,
):
    length, width = k_ref.shape
    tail = tail_ref[...]
    xn_ref[0:HALO] = jnp.where(sp_ref[0] > 0, tail, jnp.zeros_like(tail))
    xn_ref[HALO:] = rows_ref[...]
    gather_two(fs_ref[0], (w0_ref, w1_ref, w2_ref, w3_ref), w_scr)
    raw = dot(xn_ref[...], w_scr[...])
    keys = unit_rows(short_conv(raw[:, :width], taps_ref[1], length, k_scr))
    values = short_conv(raw[:, width:], taps_ref[2], length, v_scr)
    k_ref[...] = keys
    beta = beta_ref[...]
    gc = gc_ref[...]
    kb = keys * beta
    r = lax.broadcasted_iota(jnp.int32, (length, length), 0)
    c = lax.broadcasted_iota(jnp.int32, (length, length), 1)
    corr = jnp.where(r > c, dot3(kb, keys, ((1,), (1,))) * decay_ref[...], 0.0)
    half = length // 2
    first, second = inverse_unit_lower(
        [corr[:half, :half], corr[half:, half:]], half
    )
    rhs = jnp.concatenate([values * beta, kb * jnp.exp(gc)], axis=1)
    top = dot1(first, rhs[:half])
    bottom = dot1(second, rhs[half:] - dot1(corr[half:, :half], top))
    uw_ref[0:half] = top
    uw_ref[half:] = bottom
    last = gc[length - 1 : length, :]
    kd = keys * jnp.exp(last - gc)
    made = dot1(kd, uw_ref[...], ((0,), (0,)))
    ri = lax.broadcasted_iota(jnp.int32, (width, width), 0)
    ci = lax.broadcasted_iota(jnp.int32, (width, width), 1)
    linear = jnp.where(ri == ci, jnp.exp(last), 0.0) - made[:, width:]
    ab_ref[:, :width] = linear.astype(BF16)
    ab_ref[:, width:] = made[:, :width].astype(BF16)


def step_map(later, earlier, width):
    moved = dot(later[:, :width], earlier)
    offset = later[:, width:].astype(F32)
    return jnp.concatenate([moved[:, :width], moved[:, width:] + offset], axis=1)


def pair_map_kernel(sp_ref, tp_ref, fs_ref, own_ref, other_ref, pair_ref, before_ref):
    width = own_ref.shape[0]
    odd = sp_ref[0] % 2 == 1
    own, other = own_ref[...], other_ref[...]
    earlier = jnp.where(odd, other, own)
    later = jnp.where(odd, own, other)
    pair_ref[...] = step_map(later, earlier, width).astype(BF16)
    r = lax.broadcasted_iota(jnp.int32, (width, 2 * width), 0)
    c = lax.broadcasted_iota(jnp.int32, (width, 2 * width), 1)
    before_ref[...] = jnp.where(odd, other, jnp.where(r == c, 1.0, 0.0).astype(BF16))


def group_kernel(
    sp_ref, tp_ref, fs_ref, own_ref, other_ref, inner_ref,
    total_ref, linear_ref, offset_ref, before_ref,
):
    width = own_ref.shape[0]
    upper = (sp_ref[0] // 2) % 2 == 1
    own, other = own_ref[...], other_ref[...]
    earlier = jnp.where(upper, other, own)
    later = jnp.where(upper, own, other)
    total = step_map(later, earlier, width).astype(BF16)
    total_ref[...] = total
    linear_ref[...] = total[:, :width]
    offset_ref[...] = total[:, width:]
    inner = inner_ref[...]
    behind = step_map(inner, other, width)
    before_ref[...] = jnp.where(upper, behind, inner.astype(F32))


def apply(linear, state):
    high, low = split(state)
    return dot(linear, high) + dot(linear, low)


def output_kernel(
    sp_ref, tp_ref, fs_ref, xn_ref, w0_ref, w1_ref, w2_ref, w3_ref, taps_ref, gc_ref, decay_ref,
    k_ref, uw_ref, mix_ref, scale_ref, t4_ref, a8_ref, b8_ref, b12_ref, before_ref, gain_ref,
    mine_ref, other_ref,
    w_scr, w_all, q_scr, a_scr, b_scr,
):
    length, width = k_ref.shape
    pieces = (w0_ref, w1_ref, w2_ref, w3_ref)
    state = dot(a8_ref[...], b12_ref[...]) + b8_ref[...].astype(F32)
    state = apply(t4_ref[:, :width], state) + t4_ref[:, width:].astype(F32)
    state = dot3(before_ref[:, :width], state) + before_ref[:, width:]
    gather_two(fs_ref[0], pieces, w_scr)
    count, part, _ = w0_ref.shape
    skip = width // 2
    part = part - skip
    for d, piece in enumerate(pieces):
        at = pl.multiple_of(((fs_ref[0] + 4 - d) % 4) * part, 32)
        for s in range(count):
            w_all[pl.ds(at, part), s * width : (s + 1) * width] = piece[s, skip:]
    for s in range(count):
        w_scr[s * width : (s + 1) * width, 2 * width :] = w_all[
            0:width, s * width : (s + 1) * width
        ]
    raw = dot(xn_ref[...], w_scr[...])
    query = unit_rows(short_conv(raw[:, :width], taps_ref[0], length, q_scr)) * width ** (-0.5)
    silu_gate = jax.nn.silu(raw[HALO:, width : 2 * width].astype(BF16).astype(F32))
    scores = dot1(query, k_ref[...], ((1,), (1,))) * decay_ref[...]
    both = dot1(scores, uw_ref[...])
    effect = query * jnp.exp(gc_ref[...]) - both[:, width:]
    attended = both[:, :width] + dot1(effect, state)
    scale = lax.rsqrt(jnp.mean(attended * attended, axis=-1, keepdims=True) + EPS)
    delta = (attended * scale * gain_ref[...] * silu_gate).astype(BF16)
    x = raw[:, 2 * width :].astype(BF16).astype(F32)
    kind = tp_ref[0] % 4
    total = HALO + length
    a_scr[0:HALO] = jnp.zeros((HALO, width), F32)
    b_scr[0:HALO] = jnp.zeros((HALO, width), F32)
    a_scr[HALO:] = x
    two = x + a_scr[HALO - 1 : HALO - 1 + total]
    b_scr[HALO:] = two
    four = two + b_scr[HALO - 2 : HALO - 2 + total]
    a_scr[HALO:] = four
    eight = four + a_scr[HALO - 4 : HALO - 4 + total]
    b_scr[HALO:] = eight
    sixteen = eight + b_scr[HALO - 8 : HALO - 8 + total]
    window = jnp.where(
        kind == 0, two, jnp.where(kind == 1, four, jnp.where(kind == 2, eight, sixteen))
    )
    window = window[HALO:]
    place = sp_ref[0] * length + lax.broadcasted_iota(jnp.int32, (length, width), 0)
    span = jnp.where(kind == 0, 2, jnp.where(kind == 1, 4, jnp.where(kind == 2, 8, 16)))
    counts = jnp.minimum(place + 1, span).astype(F32)
    pooled = (window / counts - x[HALO:]).astype(BF16)
    pool_out = (dot(pooled, mix_ref[...]) * scale_ref[...]).astype(BF16)
    channels = jnp.concatenate([pool_out, delta], axis=1)
    core = tp_ref[0] % 2
    chips, rows, cols = mine_ref.shape
    step = 512
    for at in range(0, cols, step):
        made = dot(channels, w_all[width:, at : at + step]).astype(BF16)
        for j in range(chips):
            even = made[2 * j * rows : (2 * j + 1) * rows]
            odd = made[(2 * j + 1) * rows : (2 * j + 2) * rows]
            mine_ref[j, :, at : at + step] = jnp.where(core == 0, even, odd)
            other_ref[j, :, at : at + step] = jnp.where(core == 0, odd, even)


def pair_kernel(mine_ref, theirs_ref, out_ref):
    out_ref[...] = (mine_ref[...].astype(F32) + theirs_ref[...].astype(F32)).astype(BF16)


def sum_kernel(in_ref, out_ref):
    total = in_ref[0].astype(F32)
    for j in range(1, in_ref.shape[0]):
        total = total + in_ref[j].astype(F32)
    out_ref[...] = total.astype(BF16)


def layer(
    tokens,
    norm_gain,
    w_pool_in,
    w_query,
    w_key,
    w_value,
    w_gate,
    w_beta,
    w_decay,
    conv_weight,
    a_log,
    decay_extra,
    w_mix,
    pool_scale,
    delta_gain,
    w_out_pool,
    w_out_delta,
):
    n_sp = lax.axis_size("sp")
    n_tp = lax.axis_size("tp")
    sp_id = lax.axis_index("sp").astype(jnp.int32)
    tp_id = lax.axis_index("tp").astype(jnp.int32)
    fs_id = lax.axis_index("fs").astype(jnp.int32)
    ids = (sp_id[None], tp_id[None], fs_id[None])
    depth, width = w_key.shape
    rows, model = tokens.shape
    length = rows * n_tp
    half = depth // 2

    copies, part = call(
        start_kernel,
        (shape(n_tp, rows, model, dtype=BF16), shape(7 * depth // 4, width, dtype=BF16)),
        *ids, tokens, norm_gain,
        w_key, w_value, w_query, w_gate, w_pool_in, w_out_pool, w_out_delta,
        scratch=[pltpu.VMEM((3 * depth, width), BF16)], vmem=None,
    )
    all_rows = exchange(copies, "tp").reshape(length, model)
    tail = lax.ppermute(
        all_rows[length - HALO :], "sp", [(i, i + 1) for i in range(n_sp - 1)]
    )
    quarters = lax.all_gather(part, "sp", axis=0)
    kv = turns(quarters[:, :half], "fs", 4)
    rest = turns(quarters[:, half:], "fs", 4)

    beta, gc, decay = call(
        gate_kernel,
        (
            shape(length, 128),
            shape(length, 128),
            shape(length, length),
        ),
        *ids, a_log, all_rows, w_beta.T, w_decay.T, decay_extra.T,
        smem=4, flops=2 * length * model * 128,
    )
    ab, keys, uw, xn = call(
        local_kernel,
        (
            shape(width, 2 * width, dtype=BF16),
            shape(length, width),
            shape(length, 2 * width),
            shape(HALO + length, model, dtype=BF16),
        ),
        *ids, all_rows, tail, *kv, conv_weight, beta, gc, decay,
        scratch=[
            pltpu.VMEM((model, 2 * width), BF16),
            pltpu.VMEM((HALO + length, width), F32),
            pltpu.VMEM((HALO + length, width), F32),
        ],
        flops=20 * length * model * width,
    )
    quad = 4

    def meet(x, distance):
        return lax.ppermute(x, "sp", [(i, i ^ distance) for i in range(n_sp)])

    pair, inner = call(
        pair_map_kernel,
        (shape(width, 2 * width, dtype=BF16), shape(width, 2 * width, dtype=BF16)),
        *ids, ab, meet(ab, 1),
        flops=20 * width**3,
    )
    total, linear, offset, before = call(
        group_kernel,
        (
            shape(width, 2 * width, dtype=BF16),
            shape(width, width, dtype=BF16),
            shape(width, width, dtype=BF16),
            shape(width, 2 * width),
        ),
        *ids, pair, meet(pair, 2), inner,
        flops=20 * width**3,
    )

    def from_behind(x, first, last, distance):
        return lax.ppermute(x, "sp", [(i, i + distance) for i in range(first, last)])

    t4 = from_behind(total, 0, n_sp - quad, quad)
    b8 = from_behind(offset, 0, n_sp - 2 * quad, 2 * quad)
    a8 = from_behind(linear, quad, n_sp - 2 * quad, 2 * quad)
    b12 = from_behind(offset, 0, n_sp - 3 * quad, 3 * quad)

    chips = n_tp // 2
    mine, other = call(
        output_kernel,
        (shape(chips, rows, model, dtype=BF16), shape(chips, rows, model, dtype=BF16)),
        *ids, xn, *rest, conv_weight, gc, decay, keys, uw, w_mix[0], pool_scale.reshape(1, width),
        t4, a8, b8, b12, before, delta_gain.reshape(1, width),
        scratch=[
            pltpu.VMEM((model, 3 * width), BF16),
            pltpu.VMEM((3 * width, model), BF16),
            pltpu.VMEM((HALO + length, width), F32),
            pltpu.VMEM((2 * HALO + length, width), F32),
            pltpu.VMEM((2 * HALO + length, width), F32),
        ],
        flops=20 * length * model * width,
    )
    theirs = lax.ppermute(other, "tp", [(i, i ^ 1) for i in range(n_tp)])
    partial = call(
        pair_kernel, shape(chips, rows, model, dtype=BF16), mine, theirs, smem=0, flops=1000000
    )
    cores = [[2 * x + c for x in range(chips)] for c in range(2)]
    arrived = exchange(partial, "tp", cores)
    return call(sum_kernel, shape(rows, model, dtype=BF16), arrived, smem=0, flops=1000000)


def solution(mesh):
    placed = (
        P(("fs", "sp", "tp"), None),
        P(),
        P("sp", "tp"),
        P("sp", "tp"),
        P("sp", "tp"),
        P("sp", "tp"),
        P("sp", "tp"),
        P(),
        P(),
        P(None, None, "tp"),
        P("tp"),
        P(("fs", "sp"), "tp"),
        P("tp", None, None),
        P("tp"),
        P(),
        P("tp", "sp"),
        P("tp", "sp"),
    )
    return jax.shard_map(
        layer,
        mesh=mesh,
        in_specs=placed,
        out_specs=P(("fs", "sp", "tp"), None),
        check_vma=False,
    )
```
